32 devices in a mesh: ep: 16 (over z, y, x), tp: 2 (over core).
Axes of the slice: x: 2, y: 2, z: 4, core: 2. Of those that a mesh axis runs over, the one named last changes fastest.
Arguments:
- tokens: bfloat16 [128, 2048], P('ep'), may hold values from -6 to 6
- mixer_norm_gain: float32 [2048], replicated, may hold values from 0.1 to 1.9
- gate_projection_weight: bfloat16 [2048, 2, 2048], P(None, 'tp', 'ep'), may hold values from -0.125 to 0.125
- value_projection_weight: bfloat16 [2048, 2, 2048], P(None, 'tp', 'ep'), may hold values from -0.125 to 0.125
- input_projection_weight: bfloat16 [2048, 1024], P(None, 'tp'), may hold values from -0.125 to 0.125
- output_projection_weight: bfloat16 [2048, 1024], P(None, 'tp'), may hold values from -0.125 to 0.125
- step_projection_weight: bfloat16 [2048, 64], P(None, 'tp'), may hold values from -0.125 to 0.125
- head_step_bias: float32 [64], P('tp'), may hold values from -1 to 1
- head_decay_rate: float32 [64], P('tp'), may hold values from 0.02 to 3
- extra_log_decay: float32 [128, 64], P('ep', 'tp'), may hold values from -0.7 to 0
- value_taps: float32 [4, 4096], P(None, 'tp'), may hold values from -3 to 3
- input_taps: float32 [4, 1024], P(None, 'tp'), may hold values from -3 to 3
- output_taps: float32 [4, 1024], P(None, 'tp'), may hold values from -3 to 3
- prior_values: bfloat16 [128, 3, 4096], P('ep', None, 'tp'), may hold values from -6 to 6
- prior_input_maps: bfloat16 [128, 3, 1024], P('ep', None, 'tp'), may hold values from -6 to 6
- prior_output_maps: bfloat16 [128, 3, 1024], P('ep', None, 'tp'), may hold values from -6 to 6
- head_skip_gain: float32 [64], P('tp'), may hold values from 0.5 to 1.5
- group_norm_gain: float32 [4096], P('tp'), may hold values from 0.1 to 1.9
- mixer_output_weight: bfloat16 [4096, 2048], P('tp', 'ep'), may hold values from -0.09375 to 0.09375
- recurrent_state: float32 [128, 64, 64, 128], P('ep', 'tp'), may hold values from -6 to 6
- expert_norm_gain: float32 [2048], replicated, may hold values from 0.1 to 1.9
- routes: int32 [128, 6], P('ep'), may hold values from 0 to 15, all different within a row; in each aligned block of 8 rows (0 to 7, 8 to 15, ...) at most 4 rows name the same one
- chosen_expert_weight: float32 [128, 6], P('ep'), may hold values from 0.2 to 1
- routed_gate_weight: bfloat16 [16, 2048, 512], P('ep', None, 'tp'), may hold values from -0.125 to 0.125
- routed_up_weight: bfloat16 [16, 2048, 512], P('ep', None, 'tp'), may hold values from -0.125 to 0.125
- routed_down_weight: bfloat16 [16, 512, 2048], P('ep', 'tp'), may hold values from -0.25 to 0.25
- common_gate_weight: bfloat16 [2048, 512], P(None, 'tp'), may hold values from -0.125 to 0.125
- common_up_weight: bfloat16 [2048, 512], P(None, 'tp'), may hold values from -0.125 to 0.125
- common_down_weight: bfloat16 [512, 2048], P('tp'), may hold values from -0.25 to 0.25
Outputs:
- result: bfloat16 [128, 2048], P('ep')
- state_next: float32 [128, 64, 64, 128], P('ep', 'tp')
- next_value: bfloat16 [128, 3, 4096], P('ep', None, 'tp')
- next_input: bfloat16 [128, 3, 1024], P('ep', None, 'tp')
- next_output: bfloat16 [128, 3, 1024], P('ep', None, 'tp')
The draws below stay inside these ranges and needn't reach their ends.
Inputs may be any that keep to these rules, and one draw needn't show every extreme that they name: `routes`: the 6 experts of a row differ; among the rows of one device (aligned blocks of 8 rows) no expert is named more than 4 times.
All inputs are finite; a program needn't handle non-finite values.
Results may differ from the reference program's by a relative error of at most 0.015.
Values may be sent and summed in bfloat16 or wider, within the bound.
A program may use at most 128 MiB of HBM per device.

```python
import math
import jax
import jax.numpy as jnp
import numpy as np
from jax import lax

D = 2048
D_INNER = 4096
HEAD = 64
MIXER_HEADS = 64
STATE = 128
GROUPS = 8
CONV = 4
FE = 512
FS = 512
TOPK = 6
EXPERTS = 16
SEQ_DEV = 8
SEQUENCE_COUNT = 128
CAP = 4
HALF = 2048
N_EP = 16
N_TP = 2


def shard_levels(stream_key, dims, pieces, least, top_value):
    def one(dim, blocks):
        heights = jax.random.uniform(jax.random.fold_in(jax.random.fold_in(stream_key, 6), dim), (blocks,), jnp.float32, least / len(pieces), top_value / len(pieces))
        return jnp.repeat(jnp.exp(heights), dims[dim] // blocks).reshape((-1,) + (1,) * (len(dims) - dim - 1))

    level = one(*pieces[0])
    for cut in pieces[1:]:
        level = level * one(*cut)
    return level


def deal_out(rng, own, number, rows, amount, top, reach, slope):
    order = jax.random.permutation(rng, amount)
    crowded, ordinary = load_shares(amount, rows * top, reach, slope, True), load_shares(amount, rows * top, reach, slope, False)
    places = jnp.arange(amount)

    def named(sizes, offset_by):
        used = int((sizes > 0).sum())
        fixed = max(1, used // 4)
        passed = fixed + (places - fixed + offset_by * (used - fixed)) % max(1, amount - fixed)
        return jnp.zeros((amount,), jnp.int32).at[order[jnp.where(places < fixed, places, passed)]].set(jnp.asarray(sizes, jnp.int32))

    sizes = jnp.where(number % 4 == 0, named(crowded, number // 4), named(ordinary, number - number // 4 - 1))
    mixed = jax.random.permutation(jax.random.fold_in(own, 3), amount)
    donor, taker = mixed[0:amount // 2 * 2:2], mixed[1:amount // 2 * 2:2]
    margin = jnp.minimum(sizes[donor] - 1, reach - sizes[taker]) // 2
    margin = jnp.where((donor == order[0]) | (taker == order[0]) | (sizes[taker] == 0), 0, jnp.maximum(margin, 0))
    passed = jax.random.randint(jax.random.fold_in(own, 4), (amount // 2,), 0, 1 << 20) % (margin + 1)
    sizes = sizes.at[donor].add(-passed).at[taker].add(passed)
    items = jnp.searchsorted(jnp.cumsum(sizes), jnp.arange(rows * top), side="right").astype(jnp.int32)
    grid = items.reshape(top, rows).T
    grid = grid[jax.random.permutation(jax.random.fold_in(own, 1), rows)]
    offset_by = jax.random.randint(jax.random.fold_in(own, 2), (rows, 1), 0, top)
    return jnp.take_along_axis(grid, (jnp.arange(top)[None, :] + offset_by) % top, axis=1)


def load_shares(count, total, reach, slope, full):
    portions = [(1 << 20) // math.isqrt(standing ** slope) + 1 for standing in range(1, count + 1)]
    largest = reach if full else min(reach, max(-(-total // count), total * portions[0] // sum(portions)))
    least = 1 if total - largest >= count - 1 else 0
    given, surplus = [largest] + [least] * (count - 1), total - largest - least * (count - 1)
    while surplus > 0:
        free = [i for i in range(1, count) if given[i] < largest] or [i for i in range(1, count) if given[i] < reach]
        pool, left = sum([portions[i] for i in free]), surplus
        for i in free:
            addition = min(reach - given[i], max(1, left * portions[i] // pool), surplus)
            given[i] = given[i] + addition
            surplus = surplus - addition
    return np.array(given)


def gaussian(key, shape, spread, limit, cuts=(), kind=jnp.bfloat16):
    drawn = spread * jax.random.normal(key, shape, jnp.float32)
    if cuts:
        drawn = drawn * shard_levels(key, shape, cuts, -0.22, 0.18)
    return jnp.clip(drawn, -limit, limit).astype(kind)


def setup_inputs(seed: int = 0) -> dict:
    key_list = jax.random.split(jax.random.key(seed), 30)
    tokens = gaussian(key_list[0], (SEQUENCE_COUNT, D), 1.0, 6.0, ((0, 16),))
    mixer_norm_gain = jnp.clip(1.0 + 0.18 * jax.random.normal(key_list[1], (D,), jnp.float32), 0.1, 1.9)
    gate_projection_weight = gaussian(key_list[2], (D, N_TP, HALF), D ** -0.5, 0.125, ((1, 2), (2, 16)))
    value_projection_weight = gaussian(key_list[3], (D, N_TP, HALF), D ** -0.5, 0.125, ((1, 2), (2, 16)))
    input_projection_weight = gaussian(key_list[4], (D, GROUPS * STATE), D ** -0.5, 0.125, ((1, 2),))
    output_projection_weight = gaussian(key_list[5], (D, GROUPS * STATE), D ** -0.5, 0.125, ((1, 2),))
    step_projection_weight = gaussian(key_list[6], (D, MIXER_HEADS), D ** -0.5, 0.125, ((1, 2),))
    head_step_bias = jnp.clip(jax.random.uniform(key_list[7], (MIXER_HEADS,), jnp.float32, -1.0, 1.0) * shard_levels(key_list[7], (MIXER_HEADS,), ((0, 2),), -0.4, 0.0), -1.0, 1.0)
    head_decay_rate = jnp.clip(jnp.exp(math.log(3.0) - 5.0106353 * jax.random.uniform(key_list[8], (MIXER_HEADS,), jnp.float32) ** shard_levels(key_list[8], (MIXER_HEADS,), ((0, 2),), -0.2, 0.2)), 0.02, 3.0)
    extra_log_decay = jnp.clip(-0.7 + 0.7 * jax.random.uniform(key_list[9], (SEQUENCE_COUNT, MIXER_HEADS), jnp.float32) ** shard_levels(key_list[9], (SEQUENCE_COUNT, MIXER_HEADS), ((0, 16), (1, 2)), -0.2, 0.2), -0.7, 0.0)
    value_taps = gaussian(key_list[10], (CONV, D_INNER), 0.5, 3.0, ((1, 2),), jnp.float32)
    input_taps = gaussian(key_list[11], (CONV, GROUPS * STATE), 0.5, 3.0, ((1, 2),), jnp.float32)
    output_taps = gaussian(key_list[12], (CONV, GROUPS * STATE), 0.5, 3.0, ((1, 2),), jnp.float32)
    prior_values = gaussian(key_list[13], (SEQUENCE_COUNT, CONV - 1, D_INNER), 1.0, 6.0, ((0, 16), (2, 2)))
    prior_input_maps = gaussian(key_list[14], (SEQUENCE_COUNT, CONV - 1, GROUPS * STATE), 1.0, 6.0, ((0, 16), (2, 2)))
    prior_output_maps = gaussian(key_list[15], (SEQUENCE_COUNT, CONV - 1, GROUPS * STATE), 1.0, 6.0, ((0, 16), (2, 2)))
    head_skip_gain = jnp.clip(0.5 + 1.0 * jax.random.uniform(key_list[16], (MIXER_HEADS,), jnp.float32) ** shard_levels(key_list[16], (MIXER_HEADS,), ((0, 2),), -0.2, 0.2), 0.5, 1.5)
    group_norm_gain = jnp.clip(1.0 + 0.18 * jax.random.normal(key_list[17], (D_INNER,), jnp.float32), 0.1, 1.9)
    mixer_output_weight = gaussian(key_list[18], (D_INNER, D), D_INNER ** -0.5, 0.09375, ((0, 2), (1, 16)))
    recurrent_state = gaussian(key_list[19], (SEQUENCE_COUNT, MIXER_HEADS, HEAD, STATE), 1.0, 6.0, ((0, 16), (1, 2)), jnp.float32)
    expert_norm_gain = jnp.clip(1.0 + 0.18 * jax.random.normal(key_list[20], (D,), jnp.float32), 0.1, 1.9)
    routes_keys = jax.random.split(jax.random.fold_in(key_list[21], 1), SEQUENCE_COUNT // SEQ_DEV)
    routes_turns = jax.random.permutation(jax.random.fold_in(key_list[21], 3), SEQUENCE_COUNT // SEQ_DEV)
    routes = jax.vmap(lambda own, number: deal_out(jax.random.fold_in(key_list[21], 2), own, number, SEQ_DEV, EXPERTS, TOPK, CAP, 1))(routes_keys, routes_turns).reshape((SEQUENCE_COUNT, TOPK))
    chosen_expert_weight = jnp.clip(0.2 + 0.8 * jax.random.uniform(key_list[22], (SEQUENCE_COUNT, TOPK), jnp.float32) ** shard_levels(key_list[22], (SEQUENCE_COUNT, TOPK), ((0, 16),), -0.2, 0.2), 0.2, 1.0)
    routed_gate_weight = gaussian(key_list[23], (EXPERTS, D, FE), D ** -0.5, 0.125, ((0, 16), (2, 2)))
    routed_up_weight = gaussian(key_list[24], (EXPERTS, D, FE), D ** -0.5, 0.125, ((0, 16), (2, 2)))
    routed_down_weight = gaussian(key_list[25], (EXPERTS, FE, D), FE ** -0.5, 0.25, ((0, 16), (1, 2)))
    common_gate_weight = gaussian(key_list[26], (D, FS), D ** -0.5, 0.125, ((1, 2),))
    common_up_weight = gaussian(key_list[27], (D, FS), D ** -0.5, 0.125, ((1, 2),))
    common_down_weight = gaussian(key_list[28], (FS, D), FS ** -0.5, 0.25, ((0, 2),))
    return dict(tokens=tokens, mixer_norm_gain=mixer_norm_gain, gate_projection_weight=gate_projection_weight, value_projection_weight=value_projection_weight, input_projection_weight=input_projection_weight, output_projection_weight=output_projection_weight, step_projection_weight=step_projection_weight, head_step_bias=head_step_bias, head_decay_rate=head_decay_rate, extra_log_decay=extra_log_decay, value_taps=value_taps, input_taps=input_taps, output_taps=output_taps, prior_values=prior_values, prior_input_maps=prior_input_maps, prior_output_maps=prior_output_maps, head_skip_gain=head_skip_gain, group_norm_gain=group_norm_gain, mixer_output_weight=mixer_output_weight, recurrent_state=recurrent_state, expert_norm_gain=expert_norm_gain, routes=routes, chosen_expert_weight=chosen_expert_weight, routed_gate_weight=routed_gate_weight, routed_up_weight=routed_up_weight, routed_down_weight=routed_down_weight, common_gate_weight=common_gate_weight, common_up_weight=common_up_weight, common_down_weight=common_down_weight)


EPSILON = 1e-06

def rms_scale(values, gain_vec):
    values = values.astype(jnp.float32)
    return values * lax.rsqrt(lax.optimization_barrier(jnp.mean(values * values, axis=-1, keepdims=True)) + EPSILON) * gain_vec

def short_conv(past_rows, fresh_row, weight):
    window = jnp.concatenate([past_rows, fresh_row[:, None, :]], axis=1)
    summed = window[:, 0].astype(jnp.float32) * weight[0]
    for offset in range(1, window.shape[1]):
        summed = summed + window[:, offset].astype(jnp.float32) * weight[offset]
    return (jax.nn.silu(summed), window[:, 1:])

def state_step(state_prev, value_conv, input_conv, output_conv, timestep_size, step_decay, head_skip_gain):
    batch_rows, head_count, head_size, state_size = state_prev.shape
    per_group = head_count // (input_conv.shape[1] // state_size)
    value_heads = value_conv.reshape(batch_rows, head_count, head_size)
    input_heads = jnp.repeat(input_conv.reshape(batch_rows, -1, state_size), per_group, axis=1)
    output_heads = jnp.repeat(output_conv.reshape(batch_rows, -1, state_size), per_group, axis=1)
    state_next = step_decay[:, :, None, None] * state_prev + (timestep_size[:, :, None] * value_heads)[:, :, :, None] * input_heads[:, :, None, :]
    mixed_heads = lax.optimization_barrier(jnp.sum(state_next * output_heads[:, :, None, :], axis=-1)) + head_skip_gain[None, :, None] * value_heads
    return (state_next, mixed_heads.reshape(batch_rows, -1))

def gated_norm(mixed_flat, gate_rows, group_norm_gain, group_width):
    gated_rows = mixed_flat * jax.nn.silu(gate_rows.astype(jnp.float32))
    grouped = gated_rows.reshape(gated_rows.shape[0], -1, group_width)
    grouped = grouped * lax.rsqrt(lax.optimization_barrier(jnp.mean(grouped * grouped, axis=-1, keepdims=True)) + EPSILON)
    return (grouped.reshape(gated_rows.shape[0], -1) * group_norm_gain).astype(jnp.bfloat16)

def half_sum(left_rows, right_matrix, halves):
    span_width = left_rows.shape[1] // halves
    summed = jnp.zeros((left_rows.shape[0], right_matrix.shape[1]), jnp.float32)
    for half_index in range(halves):
        partial_value = jnp.dot(left_rows[:, half_index * span_width:(half_index + 1) * span_width], right_matrix[half_index * span_width:(half_index + 1) * span_width], preferred_element_type=jnp.float32)
        rounded = lax.optimization_barrier(partial_value.astype(jnp.bfloat16))
        summed = summed + rounded.astype(jnp.float32)
    return summed

def reference(tokens, mixer_norm_gain, gate_projection_weight, value_projection_weight, input_projection_weight, output_projection_weight, step_projection_weight, head_step_bias, head_decay_rate, extra_log_decay, value_taps, input_taps, output_taps, prior_values, prior_input_maps, prior_output_maps, head_skip_gain, group_norm_gain, mixer_output_weight, recurrent_state, expert_norm_gain, routes, chosen_expert_weight, routed_gate_weight, routed_up_weight, routed_down_weight, common_gate_weight, common_up_weight, common_down_weight):
    normed = rms_scale(tokens, mixer_norm_gain).astype(jnp.bfloat16)
    gate_rows = jnp.dot(normed, gate_projection_weight.reshape(D, D_INNER), preferred_element_type=jnp.float32).astype(jnp.bfloat16)
    value_rows = jnp.dot(normed, value_projection_weight.reshape(D, D_INNER), preferred_element_type=jnp.float32).astype(jnp.bfloat16)
    input_rows = jnp.dot(normed, input_projection_weight, preferred_element_type=jnp.float32).astype(jnp.bfloat16)
    output_rows = jnp.dot(normed, output_projection_weight, preferred_element_type=jnp.float32).astype(jnp.bfloat16)
    step_raw = jnp.dot(normed, step_projection_weight, preferred_element_type=jnp.float32)
    value_conv, next_value = short_conv(prior_values, value_rows, value_taps)
    input_conv, next_input = short_conv(prior_input_maps, input_rows, input_taps)
    output_conv, next_output = short_conv(prior_output_maps, output_rows, output_taps)
    timestep_size = jax.nn.softplus(step_raw + head_step_bias)
    step_decay = jnp.exp(-timestep_size * head_decay_rate + extra_log_decay)
    state_next, mixed_flat = state_step(recurrent_state, value_conv, input_conv, output_conv, timestep_size, step_decay, head_skip_gain)
    mixer_rows = gated_norm(mixed_flat, gate_rows, group_norm_gain, D_INNER // GROUPS)
    mixed_out = half_sum(mixer_rows, mixer_output_weight, N_TP).astype(jnp.bfloat16)
    stream = (tokens.astype(jnp.float32) + mixed_out.astype(jnp.float32)).astype(jnp.bfloat16)
    ffn_rows = rms_scale(stream, expert_norm_gain).astype(jnp.bfloat16)
    shared_hidden = (jax.nn.silu(jnp.dot(ffn_rows, common_gate_weight, preferred_element_type=jnp.float32)) * jnp.dot(ffn_rows, common_up_weight, preferred_element_type=jnp.float32)).astype(jnp.bfloat16)
    shared_out = half_sum(shared_hidden, common_down_weight, N_TP)
    flat_routes = routes.reshape(N_EP, SEQ_DEV * TOPK)
    expert_ids = jnp.arange(EXPERTS, dtype=jnp.int32)
    onehot = (flat_routes[:, :, None] == expert_ids[None, None, :]).astype(jnp.int32)
    slot_ids = lax.optimization_barrier(jnp.sum((jnp.cumsum(onehot, axis=1) - onehot) * onehot, axis=2)).astype(jnp.int32)
    device_ids = jnp.broadcast_to(jnp.arange(N_EP, dtype=jnp.int32)[:, None], flat_routes.shape)
    token_ids = device_ids * SEQ_DEV + jnp.broadcast_to(jnp.arange(SEQ_DEV * TOPK, dtype=jnp.int32)[None, :] // TOPK, flat_routes.shape)
    slot_table = jnp.full((EXPERTS, N_EP, CAP), SEQUENCE_COUNT, jnp.int32).at[flat_routes, device_ids, slot_ids].set(token_ids)
    padded = jnp.concatenate([ffn_rows, jnp.zeros((1, D), jnp.bfloat16)], axis=0)

    def per_expert(operands):
        index_table, gate_mat, up_mat, down_mat = operands
        picked_rows = padded[index_table.reshape(-1)]
        hidden = (jax.nn.silu(jnp.dot(picked_rows, gate_mat, preferred_element_type=jnp.float32)) * jnp.dot(picked_rows, up_mat, preferred_element_type=jnp.float32)).astype(jnp.bfloat16)
        return half_sum(hidden, down_mat, N_TP).astype(jnp.bfloat16).reshape(N_EP, CAP, D)
    expert_out = lax.map(per_expert, (slot_table, routed_gate_weight, routed_up_weight, routed_down_weight))
    picked = expert_out[flat_routes, device_ids, slot_ids].astype(jnp.float32)
    weighted = picked * chosen_expert_weight.reshape(N_EP, SEQ_DEV * TOPK)[:, :, None]
    routed = lax.optimization_barrier(jnp.sum(weighted.reshape(SEQUENCE_COUNT, TOPK, D), axis=1))
    result = (stream.astype(jnp.float32) + shared_out + routed).astype(jnp.bfloat16)
    return (result, state_next, next_value, next_input, next_output)
```

```python
import functools

import jax
import jax.numpy as jnp
from jax import lax
from jax.experimental import pallas as pl
from jax.experimental.pallas import tpu as pltpu
from jax.sharding import PartitionSpec as P

D_INNER = 4096
GROUPS = 8


EPSILON = 1e-06


def rms_scale(values, gain_vec):
    values = values.astype(jnp.float32)
    return (
        values * lax.rsqrt(jnp.mean(values * values, axis=-1, keepdims=True) + EPSILON) * gain_vec
    )


def short_conv(past_rows, fresh_row, weight):
    window = jnp.concatenate([past_rows, fresh_row[:, None, :]], axis=1)
    summed = window[:, 0].astype(jnp.float32) * weight[0]
    for offset in range(1, window.shape[1]):
        summed = summed + window[:, offset].astype(jnp.float32) * weight[offset]
    return (jax.nn.silu(summed), window[:, 1:])


def state_step(
    state_prev, value_conv, input_conv, output_conv, timestep_size, step_decay, head_skip_gain
):
    batch_rows, head_count, head_size, state_size = state_prev.shape
    per_group = head_count // (input_conv.shape[1] // state_size)
    value_heads = value_conv.reshape(batch_rows, head_count, head_size)
    input_heads = jnp.repeat(input_conv.reshape(batch_rows, -1, state_size), per_group, axis=1)
    output_heads = jnp.repeat(output_conv.reshape(batch_rows, -1, state_size), per_group, axis=1)
    state_next = (
        step_decay[:, :, None, None] * state_prev
        + (timestep_size[:, :, None] * value_heads)[:, :, :, None] * input_heads[:, :, None, :]
    )
    mixed_heads = (
        jnp.sum(state_next * output_heads[:, :, None, :], axis=-1)
        + head_skip_gain[None, :, None] * value_heads
    )
    return (state_next, mixed_heads.reshape(batch_rows, -1))


def gated_norm(mixed_flat, gate_rows, group_norm_gain, group_width):
    gated_rows = mixed_flat * jax.nn.silu(gate_rows.astype(jnp.float32))
    grouped = gated_rows.reshape(gated_rows.shape[0], -1, group_width)
    grouped = grouped * lax.rsqrt(jnp.mean(grouped * grouped, axis=-1, keepdims=True) + EPSILON)
    return (grouped.reshape(gated_rows.shape[0], -1) * group_norm_gain).astype(jnp.bfloat16)


def expert_partial(arrived, gate_mat, up_mat, down_mat):
    gate_part = jnp.einsum("slcd,ldf->slcf", arrived, gate_mat, preferred_element_type=jnp.float32)
    up_part = jnp.einsum("slcd,ldf->slcf", arrived, up_mat, preferred_element_type=jnp.float32)
    hidden = (jax.nn.silu(gate_part) * up_part).astype(jnp.bfloat16)
    return jnp.einsum("slcf,lfd->slcd", hidden, down_mat, preferred_element_type=jnp.float32)


MESH = pl.DeviceIdType.MESH
BF16 = jnp.bfloat16
F32 = jnp.float32


def signal_all(n):
    me, t = lax.axis_index("ep"), lax.axis_index("tp")
    barrier = pltpu.get_barrier_semaphore()

    def tell(off, carry):
        p = lax.rem(me + off, n)
        pl.semaphore_signal(barrier, inc=1, device_id={"ep": p, "tp": t}, device_id_type=MESH)
        pl.semaphore_signal(barrier, inc=1, device_id={"ep": p, "tp": 1 - t}, device_id_type=MESH)
        return carry

    lax.fori_loop(1, n, tell, 0)
    pl.semaphore_signal(barrier, inc=1, device_id={"ep": me, "tp": 1 - t}, device_id_type=MESH)


def wait_all(n):
    pl.semaphore_wait(pltpu.get_barrier_semaphore(), 2 * n - 1)


def ep_send(n, source, target, send_sem, recv_sem):
    me, t = lax.axis_index("ep"), lax.axis_index("tp")

    def start(off, carry):
        p = lax.rem(me + off, n)
        pltpu.make_async_remote_copy(
            source(p), target(me), send_sem.at[off], recv_sem.at[me],
            device_id={"ep": p, "tp": t}, device_id_type=MESH,
        ).start()
        return carry

    lax.fori_loop(1, n, start, 0)


def ep_wait(n, target, send_sem, recv_sem, sends):
    me, t = lax.axis_index("ep"), lax.axis_index("tp")

    def finish(off, carry):
        p = lax.rem(me + n - off, n)
        copy = pltpu.make_async_remote_copy(
            target(p), target(p), send_sem.at[off], recv_sem.at[p],
            device_id={"ep": p, "tp": t}, device_id_type=MESH,
        )
        if sends:
            copy.wait_send()
        else:
            copy.wait_recv()
        return carry

    lax.fori_loop(1, n, finish, 0)


def partner_copy(source, target, send_sem, recv_sem):
    me, t = lax.axis_index("ep"), lax.axis_index("tp")
    return pltpu.make_async_remote_copy(
        source, target, send_sem, recv_sem,
        device_id={"ep": me, "tp": 1 - t}, device_id_type=MESH,
    )


def short_conv_in(past, fresh, taps, window):
    summed = past[0].astype(F32) * taps[0:1]
    for offset in range(1, past.shape[0]):
        summed = summed + past[offset].astype(F32) * taps[offset : offset + 1]
        window[offset - 1] = past[offset]
    window[past.shape[0] - 1] = fresh
    return jax.nn.silu(summed + fresh.astype(F32) * taps[past.shape[0] : past.shape[0] + 1])


def step_kernel(
    n, capacity,
    tokens, gain, step_bias, decay_rate, extra_decay, v_taps, i_taps, o_taps,
    v_past, i_past, o_past, skip, group_gain, gain2, routes, route_weight,
    state, gate_w, value_w, in_w, out_w, step_w, mix_w, cg_w, cu_w, cd_w, rg_w, ru_w, rd_w,
    result, held, v_next, i_next, o_next,
    mine, other, proj, back, old_mix, decays, columns,
    gath, part, got, out_blk, arr, ret, home, share, theirs,
    gw, vw, iw, ow, sw, wm, cg, cu, cd, rg, ru, rd,
    wsem, ssem, gs, gr, ds0, dr0, rs, rr,
    as_, ar, ps, pr, xs, xr, ds, dr, es, er, fs, fr, hs, hr,
):
    me, t = lax.axis_index("ep"), lax.axis_index("tp")
    signal_all(n)
    rows, width = tokens.shape
    half = width // 2
    piece = gate_w.shape[1]
    groups, span, states = held.shape[1:]
    inner = groups * span
    heads = step_bias.shape[1]
    per_group = heads // groups
    head = span // per_group
    pairs = (
        (gate_w, gw), (value_w, vw), (in_w, iw), (out_w, ow), (step_w, sw), (mix_w, wm),
        (cg_w, cg), (cu_w, cu), (rg_w, rg), (ru_w, ru), (rd_w, rd), (cd_w, cd),
    )
    loads = [pltpu.make_async_copy(x, y, wsem.at[i]) for i, (x, y) in enumerate(pairs)]
    reads = [pltpu.make_async_copy(state.at[r], held.at[r], ssem.at[r]) for r in range(rows)]
    for load in loads[:5] + reads + loads[5:]:
        load.start()
    normed = rms_scale(tokens[...], gain[...]).astype(BF16)
    mine[me] = jnp.where(t == 0, normed[:, :half], normed[:, half:])
    wait_all(n)
    ep_send(n, lambda p: mine.at[me], lambda p: mine.at[p], gs, gr)

    for load in loads[:5]:
        load.wait()
    in_rows = jnp.dot(normed, iw[...], preferred_element_type=F32).astype(BF16)
    out_rows = jnp.dot(normed, ow[...], preferred_element_type=F32).astype(BF16)
    step_raw = lax.dot_general(
        normed, sw[...], (((1,), (1,)), ((), ())), preferred_element_type=F32
    ) + step_bias[...]
    in_conv = short_conv_in(i_past, in_rows, i_taps, i_next)
    out_conv = short_conv_in(o_past, out_rows, o_taps, o_next)
    step = jnp.maximum(step_raw, 0.0) + jnp.log1p(jnp.exp(-jnp.abs(step_raw)))
    decay = jnp.exp(-step * decay_rate[...] + extra_decay[...])
    decays[...] = decay
    own_head = lax.broadcasted_iota(jnp.int32, (heads, inner), 0)
    of_channel = lax.div(lax.broadcasted_iota(jnp.int32, (heads, inner), 1), head)
    spread_heads = jnp.where(own_head == of_channel, 1.0, 0.0).astype(F32)
    stacked = jnp.concatenate(
        [step, decay, jnp.broadcast_to(skip[...], (rows, heads))], axis=0
    )
    wide = jnp.dot(
        stacked, spread_heads, precision=lax.Precision.HIGHEST, preferred_element_type=F32
    )
    step_wide, decay_wide, skip_wide = wide[:rows], wide[rows : 2 * rows], wide[2 * rows :]

    lane = lax.broadcasted_iota(jnp.int32, (rows, n * rows), 1)
    lane_expert, lane_slot = lax.div(lane, rows), lax.rem(lane, capacity)
    named = jnp.zeros((rows, n * rows), F32)
    weighted = jnp.zeros((rows, n * rows), F32)
    for k in range(routes.shape[1]):
        hit = routes[:, k : k + 1] == lane_expert
        named = named + jnp.where(hit, 1.0, 0.0)
        weighted = weighted + jnp.where(hit, route_weight[:, k : k + 1], 0.0)
    row_id = lax.broadcasted_iota(jnp.int32, (rows, n * rows), 0)
    earlier = jnp.zeros((rows, n * rows), F32)
    for r in range(rows - 1):
        earlier = earlier + jnp.where(row_id > r, named[r : r + 1], 0.0)
    filled = jnp.where(earlier == lane_slot.astype(F32), named, 0.0)
    spread = jnp.transpose(filled).astype(BF16)
    low_lane = lax.rem(lane, rows) < capacity
    weighted = weighted * filled
    combine = jnp.concatenate(
        [jnp.where(low_lane, weighted, 0.0), jnp.where(low_lane, 0.0, weighted)], axis=0
    )

    ep_wait(n, lambda p: mine.at[p], gs, gr, False)
    cross = partner_copy(mine, other, ds0, dr0)
    cross.start()

    def product(block_ref, start):
        block = block_ref[...].reshape(n * rows, half)
        return [
            jnp.dot(block, w[pl.ds(start, half)], preferred_element_type=F32) for w in (gw, vw)
        ]

    first = product(mine, pl.multiple_of(t * half, half))
    cross.wait_recv()
    second = product(other, pl.multiple_of((1 - t) * half, half))
    for k in range(2):
        proj[:, k] = (first[k] + second[k]).astype(BF16).reshape(n, rows, piece)
    back[me] = proj[me]
    ep_send(n, lambda p: proj.at[p], lambda p: back.at[p], rs, rr)

    for read in reads:
        read.wait()
    span_row = lax.broadcasted_iota(jnp.int32, (rows, span), 0)
    for g in range(groups):
        maps = out_conv[:, g * states : (g + 1) * states].astype(BF16)

        def reduce_row(r, acc, g=g, maps=maps):
            block = held[r, g].astype(BF16)
            sums = lax.dot_general(
                maps, block, (((1,), (1,)), ((), ())), preferred_element_type=F32
            )
            return jnp.where(span_row == r, sums, acc)

        old_mix[:, g * span : (g + 1) * span] = lax.fori_loop(
            0, rows, reduce_row, jnp.zeros((rows, span), F32)
        )

    ep_wait(n, lambda p: back.at[p], rs, rr, False)
    gate_rows = jnp.concatenate([back[j, 0] for j in range(n)], axis=1).astype(F32)
    value_rows = jnp.concatenate([back[j, 1] for j in range(n)], axis=1)
    value_conv = short_conv_in(v_past, value_rows, v_taps, v_next)
    scaled = step_wide * value_conv
    gate = jax.nn.silu(gate_rows)
    for g in range(groups):
        cut, maps = slice(g * span, (g + 1) * span), slice(g * states, (g + 1) * states)
        overlap = jnp.sum(in_conv[:, maps] * out_conv[:, maps], axis=-1, keepdims=True)
        mix = (
            decay_wide[:, cut] * old_mix[:, cut]
            + scaled[:, cut] * overlap
            + skip_wide[:, cut] * value_conv[:, cut]
        ) * gate[:, cut]
        mix = mix * lax.rsqrt(jnp.mean(mix * mix, axis=-1, keepdims=True) + EPSILON)
        gath[me, :, cut] = (mix * group_gain[:, cut]).astype(BF16)
    ep_send(n, lambda p: gath.at[me], lambda p: gath.at[p], as_, ar)

    top = scaled.astype(BF16).astype(F32)
    rest = scaled - top
    columns[...] = jnp.transpose(jnp.concatenate([top, rest, top], axis=0)).astype(BF16)
    map_row = lax.rem(lax.broadcasted_iota(jnp.int32, (3 * rows, states), 0), rows)

    def update_row(r, carry):
        decay_row = decays[pl.ds(r, 1), :]
        for g in range(groups):
            maps = in_conv[:, g * states : (g + 1) * states]
            high = maps.astype(BF16).astype(F32)
            triple = jnp.concatenate([high, high, maps - high], axis=0)
            picked = jnp.where(map_row == r, triple, 0.0).astype(BF16)
            grown = jnp.dot(
                columns[g * span : (g + 1) * span, :], picked, preferred_element_type=F32
            )
            for h in range(per_group):
                at = slice(h * head, (h + 1) * head)
                factor = decay_row[:, g * per_group + h : g * per_group + h + 1]
                held[r, g, at, :] = held[r, g, at, :] * factor + grown[at]
        return carry

    lax.fori_loop(0, rows, update_row, 0)
    for load in loads[5:]:
        load.wait()
    ep_wait(n, lambda p: gath.at[p], as_, ar, False)
    summed = jnp.dot(
        gath[...].reshape(n * rows, inner), wm[...], preferred_element_type=F32
    )
    part[...] = summed.astype(BF16).reshape(n, rows, piece)
    got[t, me] = part[me]

    def start(off, carry):
        p = lax.rem(me + off, n)
        pltpu.make_async_remote_copy(
            part.at[p], got.at[t, me], ps.at[off], pr.at[me],
            device_id={"ep": p, "tp": t}, device_id_type=MESH,
        ).start()
        pltpu.make_async_remote_copy(
            part.at[p], got.at[t, me], xs.at[off], xr.at[me],
            device_id={"ep": p, "tp": 1 - t}, device_id_type=MESH,
        ).start()
        return carry

    lax.fori_loop(1, n, start, 0)
    near = partner_copy(part.at[me], got.at[t, me], ds, dr)
    near.start()
    near_in = partner_copy(part.at[me], got.at[1 - t, me], ds, dr)
    near_in.wait_recv()
    ep_wait(n, lambda p: got.at[t, p], ps, pr, False)
    ep_wait(n, lambda p: got.at[1 - t, p], xs, xr, False)
    both = (got[0].astype(F32) + got[1].astype(F32)).astype(BF16).astype(F32)
    mixed_out = jnp.concatenate([both[j] for j in range(n)], axis=1)
    stream = (tokens[...].astype(F32) + mixed_out).astype(BF16)
    ffn = rms_scale(stream, gain2[...]).astype(BF16)

    upper = lax.rem(lax.broadcasted_iota(jnp.int32, (n * rows, 1), 0), rows) >= rows // 2
    left = jnp.dot(spread, ffn[:, :half], preferred_element_type=F32)
    right = jnp.dot(spread, ffn[:, half:], preferred_element_type=F32)
    out_blk[...] = jnp.where(upper, right, left).astype(BF16).reshape(n, rows, half)
    arr[me] = out_blk[me]
    ep_send(n, lambda p: out_blk.at[p], lambda p: arr.at[p], es, er)
    shared_hidden = (
        jax.nn.silu(jnp.dot(ffn, cg[...], preferred_element_type=F32))
        * jnp.dot(ffn, cu[...], preferred_element_type=F32)
    ).astype(BF16)
    shared = jnp.dot(shared_hidden, cd[...], preferred_element_type=F32)
    ep_wait(n, lambda p: arr.at[p], es, er, False)

    arrived = arr[...].reshape(n * rows, half)

    def up(w):
        low = jnp.dot(arrived, w[:half], preferred_element_type=F32)
        high = jnp.dot(arrived, w[half:], preferred_element_type=F32)
        count = n * rows
        other = jnp.where(
            upper, pltpu.roll(low, rows // 2, 0), pltpu.roll(high, count - rows // 2, 0)
        )
        return jnp.where(upper, high, low) + other

    hidden = (jax.nn.silu(up(rg)) * up(ru)).astype(BF16)
    out_left = jnp.dot(hidden, rd[:, :half], preferred_element_type=F32)
    out_right = jnp.dot(hidden, rd[:, half:], preferred_element_type=F32)
    ret[...] = jnp.where(upper, out_right, out_left).astype(BF16).reshape(n, rows, half)
    home[me] = ret[me]
    ep_send(n, lambda p: ret.at[p], lambda p: home.at[p], fs, fr)
    ep_wait(n, lambda p: home.at[p], fs, fr, False)
    routed = jnp.dot(
        combine, home[...].reshape(n * rows, half).astype(F32),
        precision=lax.Precision.HIGHEST, preferred_element_type=F32,
    )
    share[:, :half] = shared[:, :half] + routed[:rows]
    share[:, half:] = shared[:, half:] + routed[rows:]
    last = partner_copy(share, theirs, hs, hr)
    last.start()
    last.wait_recv()
    result[...] = (stream.astype(F32) + (share[...] + theirs[...])).astype(BF16)
    ep_wait(n, lambda p: gath.at[p], as_, ar, True)
    ep_wait(n, lambda p: got.at[t, p], ps, pr, True)
    ep_wait(n, lambda p: got.at[t, p], xs, xr, True)
    near.wait_send()
    ep_wait(n, lambda p: arr.at[p], es, er, True)
    ep_wait(n, lambda p: home.at[p], fs, fr, True)
    last.wait_send()
    ep_wait(n, lambda p: mine.at[p], gs, gr, True)
    cross.wait_send()
    ep_wait(n, lambda p: back.at[p], rs, rr, True)


def mixer_step(n, capacity, small, state, weights):
    rows, width = small[0].shape
    half = width // 2
    piece = weights[0].shape[1]
    inner = n * piece
    groups, span, _ = state.shape[1:]
    vmem, hbm = pl.BlockSpec(memory_space=pltpu.VMEM), pl.BlockSpec(memory_space=pl.ANY)
    dma = pltpu.SemaphoreType.DMA
    many = dma((n,))
    block = pltpu.VMEM((n, rows, half), BF16)
    pieces = pltpu.VMEM((n, 2, rows, piece), BF16)
    heads = small[2].shape[1]
    shape = jax.ShapeDtypeStruct
    mix_piece = weights[5].shape[1]
    return pl.pallas_call(
        functools.partial(step_kernel, n, capacity),
        out_shape=(
            pltpu.VMEM((rows, width), BF16),
            pltpu.VMEM(state.shape, F32),
            pltpu.VMEM(small[8].shape, BF16),
            pltpu.VMEM(small[9].shape, BF16),
            pltpu.VMEM(small[10].shape, BF16),
        ),
        in_specs=[vmem] * len(small) + [hbm] * (1 + len(weights)),
        out_specs=(vmem,) * 5,
        scratch_shapes=[
            block, block, pieces, pieces,
            pltpu.VMEM((rows, inner), F32),
            pltpu.VMEM((rows, heads), F32),
            pltpu.VMEM((inner, 3 * rows), BF16),
            pltpu.VMEM((n, rows, inner), BF16),
            pltpu.VMEM((n, rows, mix_piece), BF16),
            pltpu.VMEM((2, n, rows, mix_piece), BF16),
            block, block, block, block,
            pltpu.VMEM((rows, width), F32),
            pltpu.VMEM((rows, width), F32),
        ]
        + [pltpu.VMEM(w.shape, BF16) for w in weights[:9]]
        + [pltpu.VMEM(w.shape, BF16) for w in weights[9:]]
        + [dma((12,)), dma((rows,)), many, many, dma, dma, many, many]
        + [many] * 6 + [dma, dma] + [many] * 4 + [dma, dma],
        compiler_params=pltpu.CompilerParams(
            collective_id=0, has_side_effects=True, vmem_limit_bytes=54 << 20
        ),
    )(*small, state, *weights)


def store_kernel(count, *refs):
    inputs, outputs, sems = refs[:count], refs[count : 2 * count], refs[2 * count]
    rows = inputs[0].shape[0]
    copies = [
        pltpu.make_async_copy(inputs[0].at[r], outputs[0].at[r], sems.at[r]) for r in range(rows)
    ]
    for k in range(1, count):
        copies.append(pltpu.make_async_copy(inputs[k], outputs[k], sems.at[rows + k - 1]))
    for copy in copies:
        copy.start()
    for copy in copies:
        copy.wait()


def store(*arrays):
    count = len(arrays)
    return pl.pallas_call(
        functools.partial(store_kernel, count),
        out_shape=tuple(jax.ShapeDtypeStruct(a.shape, a.dtype) for a in arrays),
        in_specs=[pl.BlockSpec(memory_space=pltpu.VMEM)] * count,
        out_specs=(pl.BlockSpec(memory_space=pl.ANY),) * count,
        scratch_shapes=[pltpu.SemaphoreType.DMA((arrays[0].shape[0] + count - 1,))],
        compiler_params=pltpu.CompilerParams(vmem_limit_bytes=1 << 20),
    )(*[pltpu.with_memory_space_constraint(a, pltpu.VMEM) for a in arrays])


def fast_shards(
    tokens,
    mixer_norm_gain,
    gate_projection_weight,
    value_projection_weight,
    input_projection_weight,
    output_projection_weight,
    step_projection_weight,
    head_step_bias,
    head_decay_rate,
    extra_log_decay,
    value_taps,
    input_taps,
    output_taps,
    prior_values,
    prior_input_maps,
    prior_output_maps,
    head_skip_gain,
    group_norm_gain,
    mixer_output_weight,
    recurrent_state,
    expert_norm_gain,
    routes,
    chosen_expert_weight,
    routed_gate_weight,
    routed_up_weight,
    routed_down_weight,
    common_gate_weight,
    common_up_weight,
    common_down_weight,
):
    seq_rows, model_width = tokens.shape
    ep_count = lax.axis_size("ep")
    capacity = (seq_rows * routes.shape[1] + ep_count - 1) // ep_count + 1

    def one_row(vector):
        return vector.reshape(1, -1)

    def flat(weight):
        return weight.reshape(model_width, -1)

    states = recurrent_state.shape[3]
    group_count = input_projection_weight.shape[1] // states
    small = (
        tokens, one_row(mixer_norm_gain), one_row(head_step_bias), one_row(head_decay_rate),
        extra_log_decay, value_taps, input_taps, output_taps,
        prior_values.transpose(1, 0, 2), prior_input_maps.transpose(1, 0, 2),
        prior_output_maps.transpose(1, 0, 2), one_row(head_skip_gain), one_row(group_norm_gain),
        one_row(expert_norm_gain), routes, chosen_expert_weight,
    )
    weights = (
        flat(gate_projection_weight), flat(value_projection_weight), input_projection_weight,
        output_projection_weight, step_projection_weight.T, mixer_output_weight,
        common_gate_weight, common_up_weight, common_down_weight,
        routed_gate_weight.reshape(routed_gate_weight.shape[1:]),
        routed_up_weight.reshape(routed_up_weight.shape[1:]),
        routed_down_weight.reshape(routed_down_weight.shape[1:]),
    )
    result, state_next, next_value, next_input, next_output = mixer_step(
        ep_count, capacity, small,
        recurrent_state.reshape(seq_rows, group_count, -1, states), weights,
    )
    state_next, result, next_value, next_input, next_output = store(
        state_next, result, next_value, next_input, next_output
    )
    return (
        result,
        state_next.reshape(recurrent_state.shape),
        next_value.transpose(1, 0, 2),
        next_input.transpose(1, 0, 2),
        next_output.transpose(1, 0, 2),
    )


def fits_kernels(rows, n, tp, gate_w, mix_w, routes, routed_w):
    if tp != 2 or routed_w.shape[0] != 1 or rows != 8:
        return False
    capacity = (rows * routes.shape[1] + n - 1) // n + 1
    return gate_w.shape[2] % 128 == 0 and mix_w.shape[1] % 128 == 0 and 2 * capacity == rows


def shards(
    tokens,
    mixer_norm_gain,
    gate_projection_weight,
    value_projection_weight,
    input_projection_weight,
    output_projection_weight,
    step_projection_weight,
    head_step_bias,
    head_decay_rate,
    extra_log_decay,
    value_taps,
    input_taps,
    output_taps,
    prior_values,
    prior_input_maps,
    prior_output_maps,
    head_skip_gain,
    group_norm_gain,
    mixer_output_weight,
    recurrent_state,
    expert_norm_gain,
    routes,
    chosen_expert_weight,
    routed_gate_weight,
    routed_up_weight,
    routed_down_weight,
    common_gate_weight,
    common_up_weight,
    common_down_weight,
):
    seq_rows, model_width = tokens.shape
    ep_count = lax.axis_size("ep")
    tp_count = lax.axis_size("tp")
    if fits_kernels(seq_rows, ep_count, tp_count, gate_projection_weight, mixer_output_weight, routes, routed_gate_weight):
        return fast_shards(
            tokens, mixer_norm_gain, gate_projection_weight, value_projection_weight,
            input_projection_weight, output_projection_weight, step_projection_weight,
            head_step_bias, head_decay_rate, extra_log_decay, value_taps, input_taps,
            output_taps, prior_values, prior_input_maps, prior_output_maps, head_skip_gain,
            group_norm_gain, mixer_output_weight, recurrent_state, expert_norm_gain, routes,
            chosen_expert_weight, routed_gate_weight, routed_up_weight, routed_down_weight,
            common_gate_weight, common_up_weight, common_down_weight,
        )
    tp_place = lax.axis_index("tp")
    normed = rms_scale(tokens, mixer_norm_gain).astype(jnp.bfloat16)
    both_pieces = jnp.concatenate(
        [
            gate_projection_weight.reshape(model_width, -1),
            value_projection_weight.reshape(model_width, -1),
        ],
        axis=1,
    )
    piece_width = both_pieces.shape[1] // 2
    projected = jnp.dot(
        lax.all_gather(normed, "ep", axis=0, tiled=True),
        both_pieces,
        preferred_element_type=jnp.float32,
    ).astype(jnp.bfloat16)
    returned = lax.all_to_all(projected, "ep", split_axis=0, concat_axis=1, tiled=True).reshape(
        seq_rows, ep_count, 2, piece_width
    )
    gate_rows = returned[:, :, 0].reshape(seq_rows, -1)
    value_rows = returned[:, :, 1].reshape(seq_rows, -1)
    input_rows = jnp.dot(
        normed, input_projection_weight, preferred_element_type=jnp.float32
    ).astype(jnp.bfloat16)
    output_rows = jnp.dot(
        normed, output_projection_weight, preferred_element_type=jnp.float32
    ).astype(jnp.bfloat16)
    step_raw = jnp.dot(normed, step_projection_weight, preferred_element_type=jnp.float32)
    value_conv, next_value = short_conv(prior_values, value_rows, value_taps)
    input_conv, next_input = short_conv(prior_input_maps, input_rows, input_taps)
    output_conv, next_output = short_conv(prior_output_maps, output_rows, output_taps)
    timestep_size = jax.nn.softplus(step_raw + head_step_bias)
    step_decay = jnp.exp(-timestep_size * head_decay_rate + extra_log_decay)
    state_next, mixed_flat = state_step(
        recurrent_state,
        value_conv,
        input_conv,
        output_conv,
        timestep_size,
        step_decay,
        head_skip_gain,
    )
    mixer_rows = gated_norm(mixed_flat, gate_rows, group_norm_gain, D_INNER // GROUPS)
    partial_mix = jnp.dot(
        lax.all_gather(mixer_rows, "ep", axis=0, tiled=True),
        mixer_output_weight,
        preferred_element_type=jnp.float32,
    )
    mix_share = lax.psum_scatter(
        partial_mix.reshape(ep_count, seq_rows, -1).astype(jnp.bfloat16),
        "tp",
        scatter_dimension=1,
        tiled=True,
    )
    moved_mix = lax.all_to_all(mix_share, "ep", split_axis=0, concat_axis=2, tiled=True)
    mixed_out = lax.all_gather(moved_mix, "tp", axis=1, tiled=True).reshape(seq_rows, model_width)
    stream = (tokens.astype(jnp.float32) + mixed_out.astype(jnp.float32)).astype(jnp.bfloat16)
    ffn_rows = rms_scale(stream, expert_norm_gain).astype(jnp.bfloat16)
    shared_hidden = (
        jax.nn.silu(jnp.dot(ffn_rows, common_gate_weight, preferred_element_type=jnp.float32))
        * jnp.dot(ffn_rows, common_up_weight, preferred_element_type=jnp.float32)
    ).astype(jnp.bfloat16)
    shared_out = lax.psum(
        jnp.dot(shared_hidden, common_down_weight, preferred_element_type=jnp.float32).astype(
            jnp.bfloat16
        ),
        "tp",
    ).astype(jnp.float32)
    exp_local = routed_gate_weight.shape[0]
    expert_total = exp_local * ep_count
    topk_count = routes.shape[1]
    capacity = (seq_rows * topk_count + expert_total - 1) // expert_total + 1
    slot_count = expert_total * capacity
    expert_ids = jnp.arange(expert_total, dtype=jnp.int32)
    flat_routes = routes.reshape(-1)
    onehot = (flat_routes[:, None] == expert_ids[None, :]).astype(jnp.int32)
    slot_ids = jnp.sum((jnp.cumsum(onehot, axis=0) - onehot) * onehot, axis=1)
    positions = flat_routes * capacity + slot_ids
    matches = (jnp.arange(slot_count, dtype=jnp.int32)[:, None] == positions[None, :]).reshape(
        slot_count, seq_rows, topk_count
    )
    dispatch_mat = jnp.sum(matches.astype(jnp.float32), axis=2).astype(jnp.bfloat16)
    combine_mat = jnp.sum(jnp.where(matches, chosen_expert_weight[None], 0.0), axis=2)
    outgoing = jnp.dot(dispatch_mat, ffn_rows, preferred_element_type=jnp.float32).astype(
        jnp.bfloat16
    )
    outgoing = outgoing.reshape(ep_count, exp_local, capacity, model_width)
    half_width = model_width // tp_count
    own_cols = lax.dynamic_slice_in_dim(outgoing, tp_place * half_width, half_width, 3)
    full_rows = lax.all_gather(
        lax.all_to_all(own_cols, "ep", split_axis=0, concat_axis=0, tiled=True),
        "tp",
        axis=3,
        tiled=True,
    )
    partial_out = expert_partial(
        full_rows, routed_gate_weight, routed_up_weight, routed_down_weight
    )
    share_out = lax.psum_scatter(
        partial_out.astype(jnp.bfloat16), "tp", scatter_dimension=3, tiled=True
    )
    back_half = lax.all_to_all(share_out, "ep", split_axis=0, concat_axis=0, tiled=True)
    routed_half = lax.dot_general(
        combine_mat,
        back_half.reshape(slot_count, half_width).astype(jnp.float32),
        (((0,), (0,)), ((), ())),
        precision=lax.Precision.HIGHEST,
    )
    routed = lax.all_gather(routed_half.astype(jnp.bfloat16), "tp", axis=1, tiled=True).astype(
        routed_half.dtype
    )
    result = (stream.astype(jnp.float32) + shared_out + routed).astype(jnp.bfloat16)
    return (result, state_next, next_value, next_input, next_output)


def solution(mesh):
    return jax.shard_map(
        shards,
        mesh=mesh,
        in_specs=(
            P("ep", None),
            P(),
            P(None, "tp", "ep"),
            P(None, "tp", "ep"),
            P(None, "tp"),
            P(None, "tp"),
            P(None, "tp"),
            P("tp"),
            P("tp"),
            P("ep", "tp"),
            P(None, "tp"),
            P(None, "tp"),
            P(None, "tp"),
            P("ep", None, "tp"),
            P("ep", None, "tp"),
            P("ep", None, "tp"),
            P("tp"),
            P("tp"),
            P("tp", "ep"),
            P("ep", "tp", None, None),
            P(),
            P("ep", None),
            P("ep", None),
            P("ep", None, "tp"),
            P("ep", None, "tp"),
            P("ep", "tp", None),
            P(None, "tp"),
            P(None, "tp"),
            P("tp", None),
        ),
        out_specs=(
            P("ep", None),
            P("ep", "tp", None, None),
            P("ep", None, "tp"),
            P("ep", None, "tp"),
            P("ep", None, "tp"),
        ),
        check_vma=False,
    )
```

```python
import functools

import jax
import jax.numpy as jnp
from jax import lax
from jax.experimental import pallas as pl
from jax.experimental.pallas import tpu as pltpu
from jax.sharding import PartitionSpec as P

D_INNER = 4096
GROUPS = 8


EPSILON = 1e-06


def rms_scale(values, gain_vec):
    values = values.astype(jnp.float32)
    return (
        values * lax.rsqrt(jnp.mean(values * values, axis=-1, keepdims=True) + EPSILON) * gain_vec
    )


def short_conv(past_rows, fresh_row, weight):
    window = jnp.concatenate([past_rows, fresh_row[:, None, :]], axis=1)
    summed = window[:, 0].astype(jnp.float32) * weight[0]
    for offset in range(1, window.shape[1]):
        summed = summed + window[:, offset].astype(jnp.float32) * weight[offset]
    return (jax.nn.silu(summed), window[:, 1:])


def state_step(
    state_prev, value_conv, input_conv, output_conv, timestep_size, step_decay, head_skip_gain
):
    batch_rows, head_count, head_size, state_size = state_prev.shape
    per_group = head_count // (input_conv.shape[1] // state_size)
    value_heads = value_conv.reshape(batch_rows, head_count, head_size)
    input_heads = jnp.repeat(input_conv.reshape(batch_rows, -1, state_size), per_group, axis=1)
    output_heads = jnp.repeat(output_conv.reshape(batch_rows, -1, state_size), per_group, axis=1)
    state_next = (
        step_decay[:, :, None, None] * state_prev
        + (timestep_size[:, :, None] * value_heads)[:, :, :, None] * input_heads[:, :, None, :]
    )
    mixed_heads = (
        jnp.sum(state_next * output_heads[:, :, None, :], axis=-1)
        + head_skip_gain[None, :, None] * value_heads
    )
    return (state_next, mixed_heads.reshape(batch_rows, -1))


def gated_norm(mixed_flat, gate_rows, group_norm_gain, group_width):
    gated_rows = mixed_flat * jax.nn.silu(gate_rows.astype(jnp.float32))
    grouped = gated_rows.reshape(gated_rows.shape[0], -1, group_width)
    grouped = grouped * lax.rsqrt(jnp.mean(grouped * grouped, axis=-1, keepdims=True) + EPSILON)
    return (grouped.reshape(gated_rows.shape[0], -1) * group_norm_gain).astype(jnp.bfloat16)


def expert_partial(arrived, gate_mat, up_mat, down_mat):
    gate_part = jnp.einsum("slcd,ldf->slcf", arrived, gate_mat, preferred_element_type=jnp.float32)
    up_part = jnp.einsum("slcd,ldf->slcf", arrived, up_mat, preferred_element_type=jnp.float32)
    hidden = (jax.nn.silu(gate_part) * up_part).astype(jnp.bfloat16)
    return jnp.einsum("slcf,lfd->slcd", hidden, down_mat, preferred_element_type=jnp.float32)


MESH = pl.DeviceIdType.MESH
BF16 = jnp.bfloat16
F32 = jnp.float32
EARLY = 1
BEFORE = 4
SMALL = range(16)


def level(n):
    side = 1
    while side * side < n:
        side += 1
    return side


def line_peer(k, side):
    me = lax.axis_index("ep")
    place, spot = me // side, me % side
    upper = (2 * place) // side
    place = place + upper * (side - 1 - 2 * place)
    pick = k + (k - place + side) // side
    return (pick + upper * (side - 1 - 2 * pick)) * side + spot


def flip(spot, j):
    bit = 1
    while bit <= j:
        if j & bit:
            spot = spot + bit * (1 - 2 * ((spot // bit) % 2))
        bit *= 2
    return spot


def plane_peer(j, side, block=None):
    me = lax.axis_index("ep")
    base = me if block is None else block
    return (base // side) * side + flip(me % side, j)


def remote(source, target, send_sem, recv_sem, p, t):
    return pltpu.make_async_remote_copy(
        source, target, send_sem, recv_sem,
        device_id={"ep": p, "tp": t}, device_id_type=MESH,
    )


def signal_near(n):
    me, t = lax.axis_index("ep"), lax.axis_index("tp")
    side = level(n)
    barrier = pltpu.get_barrier_semaphore()
    for k in range(side - 1):
        for p in (line_peer(k, side), plane_peer(k + 1, side)):
            pl.semaphore_signal(barrier, inc=1, device_id={"ep": p, "tp": t}, device_id_type=MESH)
    pl.semaphore_signal(barrier, inc=1, device_id={"ep": me, "tp": 1 - t}, device_id_type=MESH)


def wait_near(n):
    pl.semaphore_wait(pltpu.get_barrier_semaphore(), 2 * (level(n) - 1) + 1)


def bulk(ref, count, send_sem, recv_sem):
    return partner_copy(ref.at[pl.ds(0, count)], ref.at[pl.ds(0, count)], send_sem, recv_sem)


def gather_start(n, ref, send_sem, line_sem, plane_sem):
    me, t = lax.axis_index("ep"), lax.axis_index("tp")
    side = level(n)
    for k in range(side - 1):
        remote(
            ref.at[me], ref.at[me], send_sem, line_sem.at[me // side], line_peer(k, side), t
        ).start()
    for j in reversed(range(1, side)):
        remote(ref.at[me], ref.at[me], send_sem, plane_sem(me), plane_peer(j, side), t).start()


def gather_forward(n, k, ref, send_sem, line_sem, plane_sem):
    t = lax.axis_index("tp")
    side = level(n)
    block = line_peer(k, side)
    bulk(ref, 1, send_sem, line_sem.at[block // side]).wait_recv()
    for j in reversed(range(1, side)):
        remote(
            ref.at[block], ref.at[block], send_sem, plane_sem(block), plane_peer(j, side), t
        ).start()


def ep_send(n, source, target, send_sem, recv_sem, also=None):
    me, t = lax.axis_index("ep"), lax.axis_index("tp")
    side = level(n)
    peers = [
        plane_peer(j, side, line_peer(k, side))
        for k in reversed(range(side - 1)) for j in reversed(range(side))
    ] + [plane_peer(j, side) for j in reversed(range(1, side))]
    for p in peers:
        remote(source(p), target(me), send_sem, recv_sem, p, t).start()
        if also is not None:
            remote(source(p), target(me), *also, p, 1 - t).start()


def partner_copy(source, target, send_sem, recv_sem):
    me, t = lax.axis_index("ep"), lax.axis_index("tp")
    return remote(source, target, send_sem, recv_sem, me, 1 - t)


def short_conv_in(past, fresh, taps, window):
    summed = past[0].astype(F32) * taps[0:1]
    for offset in range(1, past.shape[0]):
        summed = summed + past[offset].astype(F32) * taps[offset : offset + 1]
        window[offset - 1] = past[offset]
    window[past.shape[0] - 1] = fresh
    return jax.nn.silu(summed + fresh.astype(F32) * taps[past.shape[0] : past.shape[0] + 1])


def step_kernel(
    n, capacity, *refs,
):
    count = len(SMALL)
    sources, refs = refs[:count], refs[count:]
    state, *refs = refs
    weight_refs, refs = refs[:12], refs[12:]
    (result, held, v_next, i_next, o_next), refs = refs[:5], refs[5:]
    smalls, refs = refs[:count], refs[count:]
    (
        tokens, gain, step_bias, decay_rate, extra_decay, v_taps, i_taps, o_taps,
        v_past, i_past, o_past, skip, group_gain, gain2, routes, route_weight,
    ) = smalls
    (
        mine, other, proj, back, old_mix, decays, columns,
        gath, part, got, out_blk, arr, arr2, lend, borrow, ret, home,
        share, theirs, half_out, half_in,
    ), refs = refs[:21], refs[21:]
    weight_bufs, refs = refs[:12], refs[12:]
    gw, vw, iw, ow, sw, wm, cg, cu, cd, rg, ru, rd = weight_bufs
    (
        wsem, lsem, ssem, gs, gr, gp, ds0, dr0, rs, rr,
        as_, ar, ap, ps, pr, xs, xr, es, er, cs, cr, ks, kr, fs, fr, hs, hr, ls, lr,
    ) = refs
    me, t = lax.axis_index("ep"), lax.axis_index("tp")
    side = level(n)
    signal_near(n)
    rows, width = tokens.shape
    half = width // 2
    quarter = half // 2
    piece = gw.shape[1]
    groups, span, states = held.shape[1:]
    inner = groups * span
    heads = step_bias.shape[1]
    per_group = heads // groups
    head = span // per_group
    order = (2, 3, 4, 0, 1, 5, 6, 7, 9, 10, 8, 11)
    fetch = [
        pltpu.make_async_copy(x, y, lsem.at[i]) for i, (x, y) in enumerate(zip(sources, smalls))
    ]
    loads = [
        pltpu.make_async_copy(x, y, wsem.at[i])
        for i, (x, y) in enumerate(zip(weight_refs, weight_bufs))
    ]
    reads = [pltpu.make_async_copy(state, held, ssem)]
    for load in fetch + [loads[i] for i in order[:3]]:
        load.start()
    for load in fetch[:2]:
        load.wait()
    normed = rms_scale(tokens[...], gain[...]).astype(BF16)
    halves = (normed[:, :half], normed[:, half:])
    mine[me] = jnp.where(t == 0, halves[0], halves[1])
    wait_near(n)

    def own_plane(block):
        return gp.at[block // side]

    gather_start(n, mine, gs, gr, own_plane)
    for load in [loads[i] for i in order[3:5]] + reads:
        load.start()

    for load in fetch[2:]:
        load.wait()
    for i in (2, 3, 4):
        loads[i].wait()
    in_rows = jnp.dot(normed, iw[...], preferred_element_type=F32).astype(BF16)
    out_rows = jnp.dot(normed, ow[...], preferred_element_type=F32).astype(BF16)
    step_raw = lax.dot_general(
        normed, sw[...], (((1,), (1,)), ((), ())), preferred_element_type=F32
    ) + step_bias[...]
    in_conv = short_conv_in(i_past, in_rows, i_taps, i_next)
    out_conv = short_conv_in(o_past, out_rows, o_taps, o_next)
    step = jnp.maximum(step_raw, 0.0) + jnp.log1p(jnp.exp(-jnp.abs(step_raw)))
    decay = jnp.exp(-step * decay_rate[...] + extra_decay[...])
    decays[...] = decay
    own_head = lax.broadcasted_iota(jnp.int32, (heads, inner), 0)
    of_channel = lax.div(lax.broadcasted_iota(jnp.int32, (heads, inner), 1), head)
    spread_heads = jnp.where(own_head == of_channel, 1.0, 0.0).astype(F32)
    stacked = jnp.concatenate(
        [step, decay, jnp.broadcast_to(skip[...], (rows, heads))], axis=0
    )
    wide = jnp.dot(
        stacked, spread_heads, precision=lax.Precision.HIGHEST, preferred_element_type=F32
    )
    step_wide, decay_wide, skip_wide = wide[:rows], wide[rows : 2 * rows], wide[2 * rows :]

    lane = lax.broadcasted_iota(jnp.int32, (rows, n * rows), 1)
    lane_expert, lane_slot = lax.div(lane, rows), lax.rem(lane, capacity)
    named = jnp.zeros((rows, n * rows), F32)
    weighted = jnp.zeros((rows, n * rows), F32)
    for k in range(routes.shape[1]):
        hit = routes[:, k : k + 1] == lane_expert
        named = named + jnp.where(hit, 1.0, 0.0)
        weighted = weighted + jnp.where(hit, route_weight[:, k : k + 1], 0.0)
    row_id = lax.broadcasted_iota(jnp.int32, (rows, n * rows), 0)
    earlier = jnp.zeros((rows, n * rows), F32)
    for r in range(rows - 1):
        earlier = earlier + jnp.where(row_id > r, named[r : r + 1], 0.0)
    filled = jnp.where(earlier == lane_slot.astype(F32), named, 0.0)
    spread = jnp.transpose(filled).astype(BF16)
    low_lane = lax.rem(lane, rows) < capacity
    weighted = weighted * filled
    combine = jnp.concatenate(
        [jnp.where(low_lane, weighted, 0.0), jnp.where(low_lane, 0.0, weighted)], axis=0
    )


    def pass_on(block, count):
        bulk(mine, count, gs, own_plane(block)).wait_recv()
        plane = pl.ds(pl.multiple_of((block // side) * side, side), side)
        partner_copy(mine.at[plane], other.at[plane], ds0, dr0).start()

    for k in range(side - 1):
        gather_forward(n, k, mine, gs, gr, own_plane)
    pass_on(me, side - 1)

    span_row = lax.broadcasted_iota(jnp.int32, (rows, span), 0)

    def read_state(g):
        maps = out_conv[:, g * states : (g + 1) * states].astype(BF16)

        def reduce_row(r, acc):
            block = held[r, g].astype(BF16)
            sums = lax.dot_general(
                maps, block, (((1,), (1,)), ((), ())), preferred_element_type=F32
            )
            return jnp.where(span_row == r, sums, acc)

        old_mix[:, g * span : (g + 1) * span] = lax.fori_loop(
            0, rows, reduce_row, jnp.zeros((rows, span), F32)
        )

    for read in reads:
        read.wait()
    for i in order[5:]:
        loads[i].start()
    for g in range(EARLY):
        read_state(g)
    for k in range(side - 1):
        pass_on(line_peer(k, side), side - 1)

    for i in (0, 1):
        loads[i].wait()

    def product(block_ref, start):
        block = block_ref[...].reshape(n * rows, half)
        return [
            jnp.dot(block, w[pl.ds(start, half)], preferred_element_type=F32) for w in (gw, vw)
        ]

    first = product(mine, pl.multiple_of(t * half, half))

    bulk(other, n, ds0, dr0).wait_recv()
    second = product(other, pl.multiple_of((1 - t) * half, half))
    for k in range(2):
        proj[:, k] = (first[k] + second[k]).astype(BF16).reshape(n, rows, piece)
    back[me] = proj[me]
    ep_send(n, lambda p: proj.at[p], lambda p: back.at[p], rs, rr)

    for g in range(EARLY, groups):
        read_state(g)

    bulk(back, n - 1, rs, rr).wait_recv()
    gate_rows = jnp.concatenate([back[j, 0] for j in range(n)], axis=1).astype(F32)
    value_rows = jnp.concatenate([back[j, 1] for j in range(n)], axis=1)
    value_conv = short_conv_in(v_past, value_rows, v_taps, v_next)
    scaled = step_wide * value_conv
    gate = jax.nn.silu(gate_rows)
    for g in range(groups):
        cut, maps = slice(g * span, (g + 1) * span), slice(g * states, (g + 1) * states)
        overlap = jnp.sum(in_conv[:, maps] * out_conv[:, maps], axis=-1, keepdims=True)
        mix = (
            decay_wide[:, cut] * old_mix[:, cut]
            + scaled[:, cut] * overlap
            + skip_wide[:, cut] * value_conv[:, cut]
        ) * gate[:, cut]
        mix = mix * lax.rsqrt(jnp.mean(mix * mix, axis=-1, keepdims=True) + EPSILON)
        gath[me, :, cut] = (mix * group_gain[:, cut]).astype(BF16)

    def any_plane(block):
        return ap

    gather_start(n, gath, as_, ar, any_plane)

    top = scaled.astype(BF16).astype(F32)
    rest = scaled - top
    columns[...] = jnp.transpose(jnp.concatenate([top, rest, top], axis=0)).astype(BF16)
    map_row = lax.rem(lax.broadcasted_iota(jnp.int32, (3 * rows, states), 0), rows)

    def update_row(r, carry):
        decay_row = decays[pl.ds(r, 1), :]
        for g in range(groups):
            maps = in_conv[:, g * states : (g + 1) * states]
            high = maps.astype(BF16).astype(F32)
            triple = jnp.concatenate([high, high, maps - high], axis=0)
            picked = jnp.where(map_row == r, triple, 0.0).astype(BF16)
            grown = jnp.dot(
                columns[g * span : (g + 1) * span, :], picked, preferred_element_type=F32
            )
            for h in range(per_group):
                at = slice(h * head, (h + 1) * head)
                factor = decay_row[:, g * per_group + h : g * per_group + h + 1]
                held[r, g, at, :] = held[r, g, at, :] * factor + grown[at]
        return carry

    lax.fori_loop(0, BEFORE, update_row, 0)
    gather_forward(n, 0, gath, as_, ar, any_plane)
    gather_forward(n, 1, gath, as_, ar, any_plane)
    gather_forward(n, 2, gath, as_, ar, any_plane)
    lax.fori_loop(BEFORE, rows, update_row, 0)
    for i in range(5, 12):
        loads[i].wait()
    bulk(mine, n - 1, gs, gs).wait_send()
    bulk(back, n - 1, rs, rr).wait_send()
    bulk(other, n, ds0, dr0).wait_send()
    bulk(gath, n - side, as_, ap).wait_recv()
    summed = jnp.dot(
        gath[...].reshape(n * rows, inner), wm[...], preferred_element_type=F32
    )
    part[...] = summed.astype(BF16).reshape(n, rows, piece)
    got[t, me] = part[me]

    partner_copy(part.at[me], got.at[t, me], xs, xr).start()
    ep_send(n, lambda p: part.at[p], lambda p: got.at[t, p], ps, pr, (xs, xr))
    bulk(gath, n - 1, as_, ap).wait_send()
    same, cross = bulk(got.at[t], n - 1, ps, pr), bulk(got.at[1 - t], n, xs, xr)
    same.wait_recv()
    cross.wait_recv()
    both = (got[0].astype(F32) + got[1].astype(F32)).astype(BF16).astype(F32)
    mixed_out = jnp.concatenate([both[j] for j in range(n)], axis=1)
    stream = (tokens[...].astype(F32) + mixed_out).astype(BF16)
    ffn = rms_scale(stream, gain2[...]).astype(BF16)

    def own_half(values):
        return jnp.where(t == 0, values[:, :half], values[:, half:])

    def far_half(values):
        return jnp.where(t == 0, values[:, half:], values[:, :half])

    upper = lax.rem(lax.broadcasted_iota(jnp.int32, (n * rows, 1), 0), rows) >= rows // 2
    ffn_own = own_half(ffn)
    left = jnp.dot(spread, ffn_own[:, :quarter], preferred_element_type=F32)
    right = jnp.dot(spread, ffn_own[:, quarter:], preferred_element_type=F32)
    out_blk[...] = jnp.where(upper, right, left).astype(BF16).reshape(n, rows, quarter)
    arr[me] = out_blk[me]
    ep_send(n, lambda p: out_blk.at[p], lambda p: arr.at[p], es, er.at[me // side])
    shared_hidden = (
        jax.nn.silu(jnp.dot(ffn, cg[...], preferred_element_type=F32))
        * jnp.dot(ffn, cu[...], preferred_element_type=F32)
    ).astype(BF16)
    shared = jnp.dot(shared_hidden, cd[...], preferred_element_type=F32)
    share[...] = far_half(shared)
    swap = partner_copy(share, theirs, hs, hr)
    swap.start()
    same.wait_send()
    cross.wait_send()

    def relay(block, count):
        bulk(arr, count, es, er.at[block // side]).wait_recv()
        plane = pl.ds(pl.multiple_of((block // side) * side, side), side)
        partner_copy(arr.at[plane], arr2.at[plane], cs, cr).start()

    relay(me, side - 1)
    for k in range(side - 1):
        relay(line_peer(k, side), side)

    def part_dots(ref, w, start):
        block = ref[...].reshape(n * rows, quarter)
        return [
            jnp.dot(
                block, w[pl.ds(pl.multiple_of(start + k * quarter, quarter), quarter)],
                preferred_element_type=F32,
            )
            for k in range(2)
        ]

    pre = [part_dots(arr, w, t * half) for w in (rg, ru)]

    bulk(arr2, n, cs, cr).wait_recv()

    def up(w, pair):
        low, high = part_dots(arr2, w, (1 - t) * half)
        low, high = low + pair[0], high + pair[1]
        count = n * rows
        swapped = jnp.where(
            upper, pltpu.roll(low, rows // 2, 0), pltpu.roll(high, count - rows // 2, 0)
        )
        return jnp.where(upper, high, low) + swapped

    hidden = (jax.nn.silu(up(rg, pre[0])) * up(ru, pre[1])).astype(BF16)

    def down(start):
        outs = [
            jnp.dot(
                hidden, rd[:, pl.ds(pl.multiple_of(start + k * quarter, quarter), quarter)],
                preferred_element_type=F32,
            )
            for k in range(2)
        ]
        return jnp.where(upper, outs[1], outs[0])

    lend[...] = down((1 - t) * half).astype(BF16).reshape(n, rows, quarter)
    loan = partner_copy(lend, borrow, ks, kr)
    loan.start()
    own = down(t * half)
    loan.wait_recv()
    ret[...] = (own + borrow[...].reshape(n * rows, quarter).astype(F32)).astype(BF16).reshape(
        n, rows, quarter
    )
    home[me] = ret[me]
    ep_send(n, lambda p: ret.at[p], lambda p: home.at[p], fs, fr)
    bulk(arr, n - 1, es, es).wait_send()
    bulk(arr2, n, cs, cr).wait_send()
    loan.wait_send()
    swap.wait_send()
    swap.wait_recv()
    base = own_half(stream.astype(F32)) + (own_half(shared) + theirs[...])
    bulk(home, n - 1, fs, fr).wait_recv()
    routed = jnp.dot(
        combine, home[...].reshape(n * rows, quarter).astype(F32),
        precision=lax.Precision.HIGHEST, preferred_element_type=F32,
    )
    routed = jnp.concatenate([routed[:rows], routed[rows:]], axis=1)
    half_out[...] = (base + routed).astype(BF16)
    last = partner_copy(half_out, half_in, ls, lr)
    last.start()
    bulk(home, n - 1, fs, fr).wait_send()
    last.wait_recv()
    mine_half, far = half_out[...], half_in[...]
    result[:, :half] = jnp.where(t == 0, mine_half, far)
    result[:, half:] = jnp.where(t == 0, far, mine_half)
    last.wait_send()


def mixer_step(n, capacity, small, state, weights):
    rows, width = small[0].shape
    half = width // 2
    piece = weights[0].shape[1]
    inner = n * piece
    groups, span, _ = state.shape[1:]
    vmem, hbm = pl.BlockSpec(memory_space=pltpu.VMEM), pl.BlockSpec(memory_space=pl.ANY)
    dma = pltpu.SemaphoreType.DMA
    many = dma((level(n),))
    block = pltpu.VMEM((n, rows, half), BF16)
    narrow = pltpu.VMEM((n, rows, half // 2), BF16)
    pieces = pltpu.VMEM((n, 2, rows, piece), BF16)
    heads = small[2].shape[1]
    mix_piece = weights[5].shape[1]
    return pl.pallas_call(
        functools.partial(step_kernel, n, capacity),
        out_shape=(
            pltpu.VMEM((rows, width), BF16),
            pltpu.VMEM(state.shape, F32),
            pltpu.VMEM(small[8].shape, BF16),
            pltpu.VMEM(small[9].shape, BF16),
            pltpu.VMEM(small[10].shape, BF16),
        ),
        in_specs=[hbm] * (len(small) + 1 + len(weights)),
        out_specs=(vmem,) * 5,
        scratch_shapes=[pltpu.VMEM(a.shape, a.dtype) for a in small]
        + [
            block, block, pieces, pieces,
            pltpu.VMEM((rows, inner), F32),
            pltpu.VMEM((rows, heads), F32),
            pltpu.VMEM((inner, 3 * rows), BF16),
            pltpu.VMEM((n, rows, inner), BF16),
            pltpu.VMEM((n, rows, mix_piece), BF16),
            pltpu.VMEM((2, n, rows, mix_piece), BF16),
            narrow, narrow, narrow, narrow, narrow, narrow, narrow,
            pltpu.VMEM((rows, half), F32),
            pltpu.VMEM((rows, half), F32),
            pltpu.VMEM((rows, half), BF16),
            pltpu.VMEM((rows, half), BF16),
        ]
        + [pltpu.VMEM(w.shape, BF16) for w in weights]
        + [dma((len(weights),)), dma((len(small),)), dma, dma, many, many]
        + [dma] * 5 + [many] + [dma] * 6 + [many] + [dma] * 10,
        compiler_params=pltpu.CompilerParams(
            collective_id=0, has_side_effects=True, vmem_limit_bytes=54 << 20
        ),
    )(*[pltpu.with_memory_space_constraint(a, pltpu.HBM) for a in (*small, state, *weights)])


def store_kernel(count, *refs):
    inputs, outputs, sems = refs[:count], refs[count : 2 * count], refs[2 * count]
    rows = inputs[0].shape[0]
    copies = [
        pltpu.make_async_copy(inputs[0].at[r], outputs[0].at[r], sems.at[r]) for r in range(rows)
    ]
    for k in range(1, count):
        copies.append(pltpu.make_async_copy(inputs[k], outputs[k], sems.at[rows + k - 1]))
    for copy in copies:
        copy.start()
    for copy in copies:
        copy.wait()


def store(*arrays):
    count = len(arrays)
    return pl.pallas_call(
        functools.partial(store_kernel, count),
        out_shape=tuple(jax.ShapeDtypeStruct(a.shape, a.dtype) for a in arrays),
        in_specs=[pl.BlockSpec(memory_space=pltpu.VMEM)] * count,
        out_specs=(pl.BlockSpec(memory_space=pl.ANY),) * count,
        scratch_shapes=[pltpu.SemaphoreType.DMA((arrays[0].shape[0] + count - 1,))],
        compiler_params=pltpu.CompilerParams(vmem_limit_bytes=1 << 20),
    )(*[pltpu.with_memory_space_constraint(a, pltpu.VMEM) for a in arrays])


def fast_shards(
    tokens,
    mixer_norm_gain,
    gate_projection_weight,
    value_projection_weight,
    input_projection_weight,
    output_projection_weight,
    step_projection_weight,
    head_step_bias,
    head_decay_rate,
    extra_log_decay,
    value_taps,
    input_taps,
    output_taps,
    prior_values,
    prior_input_maps,
    prior_output_maps,
    head_skip_gain,
    group_norm_gain,
    mixer_output_weight,
    recurrent_state,
    expert_norm_gain,
    routes,
    chosen_expert_weight,
    routed_gate_weight,
    routed_up_weight,
    routed_down_weight,
    common_gate_weight,
    common_up_weight,
    common_down_weight,
):
    seq_rows, model_width = tokens.shape
    ep_count = lax.axis_size("ep")
    capacity = (seq_rows * routes.shape[1] + ep_count - 1) // ep_count + 1

    def one_row(vector):
        return vector.reshape(1, -1)

    def flat(weight):
        return weight.reshape(model_width, -1)

    states = recurrent_state.shape[3]
    group_count = input_projection_weight.shape[1] // states
    small = (
        tokens, one_row(mixer_norm_gain), one_row(head_step_bias), one_row(head_decay_rate),
        extra_log_decay, value_taps, input_taps, output_taps,
        prior_values.transpose(1, 0, 2), prior_input_maps.transpose(1, 0, 2),
        prior_output_maps.transpose(1, 0, 2), one_row(head_skip_gain), one_row(group_norm_gain),
        one_row(expert_norm_gain), routes, chosen_expert_weight,
    )
    weights = (
        flat(gate_projection_weight), flat(value_projection_weight), input_projection_weight,
        output_projection_weight, step_projection_weight.T, mixer_output_weight,
        common_gate_weight, common_up_weight, common_down_weight,
        routed_gate_weight.reshape(routed_gate_weight.shape[1:]),
        routed_up_weight.reshape(routed_up_weight.shape[1:]),
        routed_down_weight.reshape(routed_down_weight.shape[1:]),
    )
    result, state_next, next_value, next_input, next_output = mixer_step(
        ep_count, capacity, small,
        recurrent_state.reshape(seq_rows, group_count, -1, states), weights,
    )
    state_next, result, next_value, next_input, next_output = store(
        state_next, result, next_value, next_input, next_output
    )
    return (
        result,
        state_next.reshape(recurrent_state.shape),
        next_value.transpose(1, 0, 2),
        next_input.transpose(1, 0, 2),
        next_output.transpose(1, 0, 2),
    )


def fits_kernels(rows, n, tp, gate_w, mix_w, routes, routed_w):
    if tp != 2 or routed_w.shape[0] != 1 or rows != 8:
        return False
    capacity = (rows * routes.shape[1] + n - 1) // n + 1
    return level(n) ** 2 == n and gate_w.shape[2] % 128 == 0 and mix_w.shape[1] % 128 == 0 and 2 * capacity == rows


def shards(
    tokens,
    mixer_norm_gain,
    gate_projection_weight,
    value_projection_weight,
    input_projection_weight,
    output_projection_weight,
    step_projection_weight,
    head_step_bias,
    head_decay_rate,
    extra_log_decay,
    value_taps,
    input_taps,
    output_taps,
    prior_values,
    prior_input_maps,
    prior_output_maps,
    head_skip_gain,
    group_norm_gain,
    mixer_output_weight,
    recurrent_state,
    expert_norm_gain,
    routes,
    chosen_expert_weight,
    routed_gate_weight,
    routed_up_weight,
    routed_down_weight,
    common_gate_weight,
    common_up_weight,
    common_down_weight,
):
    seq_rows, model_width = tokens.shape
    ep_count = lax.axis_size("ep")
    tp_count = lax.axis_size("tp")
    if fits_kernels(seq_rows, ep_count, tp_count, gate_projection_weight, mixer_output_weight, routes, routed_gate_weight):
        return fast_shards(
            tokens, mixer_norm_gain, gate_projection_weight, value_projection_weight,
            input_projection_weight, output_projection_weight, step_projection_weight,
            head_step_bias, head_decay_rate, extra_log_decay, value_taps, input_taps,
            output_taps, prior_values, prior_input_maps, prior_output_maps, head_skip_gain,
            group_norm_gain, mixer_output_weight, recurrent_state, expert_norm_gain, routes,
            chosen_expert_weight, routed_gate_weight, routed_up_weight, routed_down_weight,
            common_gate_weight, common_up_weight, common_down_weight,
        )
    tp_place = lax.axis_index("tp")
    normed = rms_scale(tokens, mixer_norm_gain).astype(jnp.bfloat16)
    both_pieces = jnp.concatenate(
        [
            gate_projection_weight.reshape(model_width, -1),
            value_projection_weight.reshape(model_width, -1),
        ],
        axis=1,
    )
    piece_width = both_pieces.shape[1] // 2
    projected = jnp.dot(
        lax.all_gather(normed, "ep", axis=0, tiled=True),
        both_pieces,
        preferred_element_type=jnp.float32,
    ).astype(jnp.bfloat16)
    returned = lax.all_to_all(projected, "ep", split_axis=0, concat_axis=1, tiled=True).reshape(
        seq_rows, ep_count, 2, piece_width
    )
    gate_rows = returned[:, :, 0].reshape(seq_rows, -1)
    value_rows = returned[:, :, 1].reshape(seq_rows, -1)
    input_rows = jnp.dot(
        normed, input_projection_weight, preferred_element_type=jnp.float32
    ).astype(jnp.bfloat16)
    output_rows = jnp.dot(
        normed, output_projection_weight, preferred_element_type=jnp.float32
    ).astype(jnp.bfloat16)
    step_raw = jnp.dot(normed, step_projection_weight, preferred_element_type=jnp.float32)
    value_conv, next_value = short_conv(prior_values, value_rows, value_taps)
    input_conv, next_input = short_conv(prior_input_maps, input_rows, input_taps)
    output_conv, next_output = short_conv(prior_output_maps, output_rows, output_taps)
    timestep_size = jax.nn.softplus(step_raw + head_step_bias)
    step_decay = jnp.exp(-timestep_size * head_decay_rate + extra_log_decay)
    state_next, mixed_flat = state_step(
        recurrent_state,
        value_conv,
        input_conv,
        output_conv,
        timestep_size,
        step_decay,
        head_skip_gain,
    )
    mixer_rows = gated_norm(mixed_flat, gate_rows, group_norm_gain, D_INNER // GROUPS)
    partial_mix = jnp.dot(
        lax.all_gather(mixer_rows, "ep", axis=0, tiled=True),
        mixer_output_weight,
        preferred_element_type=jnp.float32,
    )
    mix_share = lax.psum_scatter(
        partial_mix.reshape(ep_count, seq_rows, -1).astype(jnp.bfloat16),
        "tp",
        scatter_dimension=1,
        tiled=True,
    )
    moved_mix = lax.all_to_all(mix_share, "ep", split_axis=0, concat_axis=2, tiled=True)
    mixed_out = lax.all_gather(moved_mix, "tp", axis=1, tiled=True).reshape(seq_rows, model_width)
    stream = (tokens.astype(jnp.float32) + mixed_out.astype(jnp.float32)).astype(jnp.bfloat16)
    ffn_rows = rms_scale(stream, expert_norm_gain).astype(jnp.bfloat16)
    shared_hidden = (
        jax.nn.silu(jnp.dot(ffn_rows, common_gate_weight, preferred_element_type=jnp.float32))
        * jnp.dot(ffn_rows, common_up_weight, preferred_element_type=jnp.float32)
    ).astype(jnp.bfloat16)
    shared_out = lax.psum(
        jnp.dot(shared_hidden, common_down_weight, preferred_element_type=jnp.float32).astype(
            jnp.bfloat16
        ),
        "tp",
    ).astype(jnp.float32)
    exp_local = routed_gate_weight.shape[0]
    expert_total = exp_local * ep_count
    topk_count = routes.shape[1]
    capacity = (seq_rows * topk_count + expert_total - 1) // expert_total + 1
    slot_count = expert_total * capacity
    expert_ids = jnp.arange(expert_total, dtype=jnp.int32)
    flat_routes = routes.reshape(-1)
    onehot = (flat_routes[:, None] == expert_ids[None, :]).astype(jnp.int32)
    slot_ids = jnp.sum((jnp.cumsum(onehot, axis=0) - onehot) * onehot, axis=1)
    positions = flat_routes * capacity + slot_ids
    matches = (jnp.arange(slot_count, dtype=jnp.int32)[:, None] == positions[None, :]).reshape(
        slot_count, seq_rows, topk_count
    )
    dispatch_mat = jnp.sum(matches.astype(jnp.float32), axis=2).astype(jnp.bfloat16)
    combine_mat = jnp.sum(jnp.where(matches, chosen_expert_weight[None], 0.0), axis=2)
    outgoing = jnp.dot(dispatch_mat, ffn_rows, preferred_element_type=jnp.float32).astype(
        jnp.bfloat16
    )
    outgoing = outgoing.reshape(ep_count, exp_local, capacity, model_width)
    half_width = model_width // tp_count
    own_cols = lax.dynamic_slice_in_dim(outgoing, tp_place * half_width, half_width, 3)
    full_rows = lax.all_gather(
        lax.all_to_all(own_cols, "ep", split_axis=0, concat_axis=0, tiled=True),
        "tp",
        axis=3,
        tiled=True,
    )
    partial_out = expert_partial(
        full_rows, routed_gate_weight, routed_up_weight, routed_down_weight
    )
    share_out = lax.psum_scatter(
        partial_out.astype(jnp.bfloat16), "tp", scatter_dimension=3, tiled=True
    )
    back_half = lax.all_to_all(share_out, "ep", split_axis=0, concat_axis=0, tiled=True)
    routed_half = lax.dot_general(
        combine_mat,
        back_half.reshape(slot_count, half_width).astype(jnp.float32),
        (((0,), (0,)), ((), ())),
        precision=lax.Precision.HIGHEST,
    )
    routed = lax.all_gather(routed_half.astype(jnp.bfloat16), "tp", axis=1, tiled=True).astype(
        routed_half.dtype
    )
    result = (stream.astype(jnp.float32) + shared_out + routed).astype(jnp.bfloat16)
    return (result, state_next, next_value, next_input, next_output)


def solution(mesh):
    return jax.shard_map(
        shards,
        mesh=mesh,
        in_specs=(
            P("ep", None),
            P(),
            P(None, "tp", "ep"),
            P(None, "tp", "ep"),
            P(None, "tp"),
            P(None, "tp"),
            P(None, "tp"),
            P("tp"),
            P("tp"),
            P("ep", "tp"),
            P(None, "tp"),
            P(None, "tp"),
            P(None, "tp"),
            P("ep", None, "tp"),
            P("ep", None, "tp"),
            P("ep", None, "tp"),
            P("tp"),
            P("tp"),
            P("tp", "ep"),
            P("ep", "tp", None, None),
            P(),
            P("ep", None),
            P("ep", None),
            P("ep", None, "tp"),
            P("ep", None, "tp"),
            P("ep", "tp", None),
            P(None, "tp"),
            P(None, "tp"),
            P("tp", None),
        ),
        out_specs=(
            P("ep", None),
            P("ep", "tp", None, None),
            P("ep", None, "tp"),
            P("ep", None, "tp"),
            P("ep", None, "tp"),
        ),
        check_vma=False,
    )
```

```python
import functools

import jax
import jax.numpy as jnp
from jax import lax
from jax.experimental import pallas as pl
from jax.experimental.pallas import tpu as pltpu
from jax.sharding import PartitionSpec as P

D_INNER = 4096
GROUPS = 8


EPSILON = 1e-06


def rms_scale(values, gain_vec):
    values = values.astype(jnp.float32)
    return (
        values * lax.rsqrt(jnp.mean(values * values, axis=-1, keepdims=True) + EPSILON) * gain_vec
    )


def short_conv(past_rows, fresh_row, weight):
    window = jnp.concatenate([past_rows, fresh_row[:, None, :]], axis=1)
    summed = window[:, 0].astype(jnp.float32) * weight[0]
    for offset in range(1, window.shape[1]):
        summed = summed + window[:, offset].astype(jnp.float32) * weight[offset]
    return (jax.nn.silu(summed), window[:, 1:])


def state_step(
    state_prev, value_conv, input_conv, output_conv, timestep_size, step_decay, head_skip_gain
):
    batch_rows, head_count, head_size, state_size = state_prev.shape
    per_group = head_count // (input_conv.shape[1] // state_size)
    value_heads = value_conv.reshape(batch_rows, head_count, head_size)
    input_heads = jnp.repeat(input_conv.reshape(batch_rows, -1, state_size), per_group, axis=1)
    output_heads = jnp.repeat(output_conv.reshape(batch_rows, -1, state_size), per_group, axis=1)
    state_next = (
        step_decay[:, :, None, None] * state_prev
        + (timestep_size[:, :, None] * value_heads)[:, :, :, None] * input_heads[:, :, None, :]
    )
    mixed_heads = (
        jnp.sum(state_next * output_heads[:, :, None, :], axis=-1)
        + head_skip_gain[None, :, None] * value_heads
    )
    return (state_next, mixed_heads.reshape(batch_rows, -1))


def gated_norm(mixed_flat, gate_rows, group_norm_gain, group_width):
    gated_rows = mixed_flat * jax.nn.silu(gate_rows.astype(jnp.float32))
    grouped = gated_rows.reshape(gated_rows.shape[0], -1, group_width)
    grouped = grouped * lax.rsqrt(jnp.mean(grouped * grouped, axis=-1, keepdims=True) + EPSILON)
    return (grouped.reshape(gated_rows.shape[0], -1) * group_norm_gain).astype(jnp.bfloat16)


def expert_partial(arrived, gate_mat, up_mat, down_mat):
    gate_part = jnp.einsum("slcd,ldf->slcf", arrived, gate_mat, preferred_element_type=jnp.float32)
    up_part = jnp.einsum("slcd,ldf->slcf", arrived, up_mat, preferred_element_type=jnp.float32)
    hidden = (jax.nn.silu(gate_part) * up_part).astype(jnp.bfloat16)
    return jnp.einsum("slcf,lfd->slcd", hidden, down_mat, preferred_element_type=jnp.float32)


MESH = pl.DeviceIdType.MESH
BF16 = jnp.bfloat16
F32 = jnp.float32
EARLY = 1
BEFORE = 4
SMALL = range(16)
TWIN = (0, 1, 5, 9, 10, 11)


def level(n):
    side = 1
    while side * side < n:
        side += 1
    return side


def line_peer(k, side):
    me = lax.axis_index("ep")
    place, spot = me // side, me % side
    upper = (2 * place) // side
    place = place + upper * (side - 1 - 2 * place)
    pick = k + (k - place + side) // side
    return (pick + upper * (side - 1 - 2 * pick)) * side + spot


def flip(spot, j):
    bit = 1
    while bit <= j:
        if j & bit:
            spot = spot + bit * (1 - 2 * ((spot // bit) % 2))
        bit *= 2
    return spot


def plane_peer(j, side, block=None):
    me = lax.axis_index("ep")
    base = me if block is None else block
    return (base // side) * side + flip(me % side, j)


def remote(source, target, send_sem, recv_sem, p, t):
    return pltpu.make_async_remote_copy(
        source, target, send_sem, recv_sem,
        device_id={"ep": p, "tp": t}, device_id_type=MESH,
    )


def signal_near(n):
    me, t = lax.axis_index("ep"), lax.axis_index("tp")
    side = level(n)
    barrier = pltpu.get_barrier_semaphore()
    for k in range(side - 1):
        for p in (line_peer(k, side), plane_peer(k + 1, side)):
            for core in range(2):
                pl.semaphore_signal(
                    barrier, inc=1, device_id={"ep": p, "tp": core}, device_id_type=MESH
                )
    pl.semaphore_signal(barrier, inc=1, device_id={"ep": me, "tp": 1 - t}, device_id_type=MESH)


def wait_near(n):
    pl.semaphore_wait(pltpu.get_barrier_semaphore(), 4 * (level(n) - 1) + 1)


def bulk(ref, count, send_sem, recv_sem):
    return partner_copy(ref.at[pl.ds(0, count)], ref.at[pl.ds(0, count)], send_sem, recv_sem)


def gather_start(n, ref, send_sem, line_sem, plane_sem):
    me, t = lax.axis_index("ep"), lax.axis_index("tp")
    side = level(n)
    for k in range(side - 1):
        remote(
            ref.at[me], ref.at[me], send_sem, line_sem.at[me // side], line_peer(k, side), t
        ).start()
    for j in reversed(range(1, side)):
        remote(ref.at[me], ref.at[me], send_sem, plane_sem(me), plane_peer(j, side), t).start()


def gather_forward(n, k, ref, send_sem, line_sem, plane_sem):
    t = lax.axis_index("tp")
    side = level(n)
    block = line_peer(k, side)
    bulk(ref, 1, send_sem, line_sem.at[block // side]).wait_recv()
    for j in reversed(range(1, side)):
        remote(
            ref.at[block], ref.at[block], send_sem, plane_sem(block), plane_peer(j, side), t
        ).start()


def home_core(n, p):
    side = level(n)
    return (p % side) // (side // 2)


def home_spot(n, p):
    side = level(n)
    return (p // side) * (side // 2) + p % (side // 2)


def at_spot(n, i):
    side = level(n)
    half_side = side // 2
    return (i // half_side) * side + lax.axis_index("tp") * half_side + i % half_side


def is_home(n):
    return lax.axis_index("tp") == home_core(n, lax.axis_index("ep"))


def by_home(n, at_home, away):
    home = is_home(n)

    @pl.when(home)
    def _():
        at_home()

    @pl.when(jnp.logical_not(home))
    def _():
        away()


def rows_start(n, stage, rows_ref, send_sem, line_sem, plane_sem):
    me, t = lax.axis_index("ep"), lax.axis_index("tp")
    side = level(n)
    core = home_core(n, me)
    target = rows_ref.at[t, home_spot(n, me)]
    arrive = line_sem.at[(me // side) * 2 + t]
    for k in range(side - 1):
        remote(stage, target, send_sem, arrive, line_peer(k, side), core).start()
    for j in reversed(range(1, side)):
        remote(stage, target, send_sem, plane_sem, plane_peer(j, side), core).start()


def rows_forward(n, k, rows_ref, send_sem, line_sem, plane_sem):
    t = lax.axis_index("tp")
    side = level(n)

    @pl.when(is_home(n))
    def _():
        q = line_peer(k, side)
        for f in range(2):
            block = rows_ref.at[f, home_spot(n, q)]
            arrive = line_sem.at[(q // side) * 2 + f]
            partner_copy(block, block, send_sem.at[k], arrive).wait_recv()
            for j in reversed(range(1, side)):
                remote(block, block, send_sem.at[k], plane_sem, plane_peer(j, side), t).start()


def rows_wait(n, rows_ref, send_sem, plane_sem):
    def arrived(count):
        block = rows_ref.at[:, pl.ds(0, count)]
        partner_copy(block, block, send_sem, plane_sem).wait_recv()

    hn = n // 2
    by_home(n, lambda: arrived(hn - level(n)), lambda: arrived(hn))


def rows_sent(n, rows_ref, own_sem, send_sem):
    side = level(n)
    bulk(rows_ref.at[0], 2 * (side - 1), own_sem, own_sem).wait_send()

    @pl.when(is_home(n))
    def _():
        block = rows_ref.at[:, pl.ds(0, side - 1)]
        for k in range(side - 1):
            partner_copy(block, block, send_sem.at[k], send_sem.at[k]).wait_send()


def back_start(n, source, target, send_sem, recv_sem):
    me, t = lax.axis_index("ep"), lax.axis_index("tp")
    hn = n // 2
    for j in reversed(range(1, hn)):
        i = flip(home_spot(n, me), j)
        for core in range(2):
            remote(
                source.at[core, i], target.at[me], send_sem, recv_sem, at_spot(n, i), core
            ).start()
    i = home_spot(n, me)

    def at_home():
        partner_copy(source.at[1 - t, i], target.at[me], send_sem, recv_sem).start()
        target[me] = source[t, i]

    def away():
        for core in range(2):
            remote(
                source.at[core, i], target.at[me], send_sem, recv_sem, at_spot(n, i), core
            ).start()

    by_home(n, at_home, away)


def back_wait(n, target, send_sem, recv_sem):
    by_home(
        n, lambda: bulk(target, n - 1, send_sem, recv_sem).wait_recv(),
        lambda: bulk(target, n, send_sem, recv_sem).wait_recv(),
    )


def back_sent(n, target, send_sem, recv_sem):
    by_home(
        n, lambda: bulk(target, n - 1, send_sem, recv_sem).wait_send(),
        lambda: bulk(target, n, send_sem, recv_sem).wait_send(),
    )


def partner_copy(source, target, send_sem, recv_sem):
    me, t = lax.axis_index("ep"), lax.axis_index("tp")
    return remote(source, target, send_sem, recv_sem, me, 1 - t)


def short_conv_in(past, fresh, taps, window):
    summed = past[0].astype(F32) * taps[0:1]
    for offset in range(1, past.shape[0]):
        summed = summed + past[offset].astype(F32) * taps[offset : offset + 1]
        window[offset - 1] = past[offset]
    window[past.shape[0] - 1] = fresh
    return jax.nn.silu(summed + fresh.astype(F32) * taps[past.shape[0] : past.shape[0] + 1])


def step_kernel(
    n, capacity, *refs,
):
    count = len(SMALL)
    sources, refs = refs[:count], refs[count:]
    state, *refs = refs
    weight_refs, refs = refs[:12], refs[12:]
    (result, held, v_next, i_next, o_next), refs = refs[:5], refs[5:]
    smalls, refs = refs[:count], refs[count:]
    (
        tokens, gain, step_bias, decay_rate, extra_decay, v_taps, i_taps, o_taps,
        v_past, i_past, o_past, skip, group_gain, gain2, routes, route_weight,
    ) = smalls
    (
        stage, row_buf, proj, back, old_mix, decays, columns,
        mixed, gath, early_out, early_in, blocks, sx, own_rows, ret, home,
        share, theirs, half_out, half_in,
    ), refs = refs[:20], refs[20:]
    weight_bufs, refs = refs[:12], refs[12:]
    gw, vw, iw, ow, sw, wm, cg, cu, cd, rg, ru, rd = weight_bufs
    (
        wsem, lsem, ssem, ts, tr, gs, gf, gl, gp, rs, rr, es, er,
        as_, af, al, ap, ns, nr, ps, pr, pp, fs, fr, os_, or_, hs, hr, ls, lr,
    ) = refs
    me, t = lax.axis_index("ep"), lax.axis_index("tp")
    side = level(n)
    signal_near(n)
    rows, width = tokens.shape
    half = width // 2
    quarter = half // 2
    piece = gw.shape[2]
    hn = n // 2
    spot = home_spot(n, me)
    at_home = is_home(n)
    groups, span, states = held.shape[1:]
    inner = groups * span
    heads = step_bias.shape[1]
    per_group = heads // groups
    head = span // per_group
    order = (2, 3, 4, 0, 1, 5, 6, 7, 9, 10, 8, 11)
    fetch = [
        pltpu.make_async_copy(x, y, lsem.at[i]) for i, (x, y) in enumerate(zip(sources, smalls))
    ]
    loads = [
        pltpu.make_async_copy(x, y.at[t] if i in TWIN else y, wsem.at[i])
        for i, (x, y) in enumerate(zip(weight_refs, weight_bufs))
    ]
    twins = [
        partner_copy(weight_refs[i], weight_bufs[i].at[t], ts.at[k], tr.at[k])
        for k, i in enumerate(TWIN)
    ]
    reads = [pltpu.make_async_copy(state, held, ssem)]
    for load in fetch + [loads[i] for i in order[:3]]:
        load.start()
    for load in fetch[:2]:
        load.wait()
    normed = rms_scale(tokens[...], gain[...]).astype(BF16)

    def own_half(values):
        return jnp.where(t == 0, values[:, :half], values[:, half:])

    def far_half(values):
        return jnp.where(t == 0, values[:, half:], values[:, :half])

    stage[...] = own_half(normed)

    @pl.when(at_home)
    def _():
        row_buf[0, spot] = normed[:, :half]
        row_buf[1, spot] = normed[:, half:]

    wait_near(n)
    rows_start(n, stage, row_buf, gs, gl, gp)
    for twin in twins[:2]:
        twin.start()
    for load in [loads[i] for i in order[3:5]] + reads:
        load.start()

    for load in fetch[2:]:
        load.wait()
    for i in (2, 3, 4):
        loads[i].wait()
    in_rows = jnp.dot(normed, iw[...], preferred_element_type=F32).astype(BF16)
    out_rows = jnp.dot(normed, ow[...], preferred_element_type=F32).astype(BF16)
    step_raw = lax.dot_general(
        normed, sw[...], (((1,), (1,)), ((), ())), preferred_element_type=F32
    ) + step_bias[...]
    in_conv = short_conv_in(i_past, in_rows, i_taps, i_next)
    out_conv = short_conv_in(o_past, out_rows, o_taps, o_next)
    step = jnp.maximum(step_raw, 0.0) + jnp.log1p(jnp.exp(-jnp.abs(step_raw)))
    decay = jnp.exp(-step * decay_rate[...] + extra_decay[...])
    decays[...] = decay
    own_head = lax.broadcasted_iota(jnp.int32, (heads, inner), 0)
    of_channel = lax.div(lax.broadcasted_iota(jnp.int32, (heads, inner), 1), head)
    spread_heads = jnp.where(own_head == of_channel, 1.0, 0.0).astype(F32)
    stacked = jnp.concatenate(
        [step, decay, jnp.broadcast_to(skip[...], (rows, heads))], axis=0
    )
    wide = jnp.dot(
        stacked, spread_heads, precision=lax.Precision.HIGHEST, preferred_element_type=F32
    )
    step_wide, decay_wide, skip_wide = wide[:rows], wide[rows : 2 * rows], wide[2 * rows :]

    lane = lax.broadcasted_iota(jnp.int32, (rows, n * rows), 1)
    lane_expert, lane_slot = lax.div(lane, rows), lax.rem(lane, capacity)
    named = jnp.zeros((rows, n * rows), F32)
    weighted = jnp.zeros((rows, n * rows), F32)
    for k in range(routes.shape[1]):
        hit = routes[:, k : k + 1] == lane_expert
        named = named + jnp.where(hit, 1.0, 0.0)
        weighted = weighted + jnp.where(hit, route_weight[:, k : k + 1], 0.0)
    row_id = lax.broadcasted_iota(jnp.int32, (rows, n * rows), 0)
    earlier = jnp.zeros((rows, n * rows), F32)
    for r in range(rows - 1):
        earlier = earlier + jnp.where(row_id > r, named[r : r + 1], 0.0)
    filled = jnp.where(earlier == lane_slot.astype(F32), named, 0.0)
    spread = jnp.transpose(filled).astype(BF16)
    low_lane = lax.rem(lane, rows) < capacity
    weighted = weighted * filled
    combine = jnp.concatenate(
        [jnp.where(low_lane, weighted, 0.0), jnp.where(low_lane, 0.0, weighted)], axis=0
    )

    place = jnp.where(
        lax.broadcasted_iota(jnp.int32, (rows, piece), 1)
        == lax.broadcasted_iota(jnp.int32, (rows, piece), 0) + spot * rows,
        1.0, 0.0,
    ).astype(BF16)
    picks = jnp.dot(spread, place, preferred_element_type=F32).astype(BF16)
    early_out[:, 1] = picks.reshape(n, rows, piece)
    for c in range(n):
        early_out[c, 0] = tokens[:, c * piece : (c + 1) * piece]

    @pl.when(at_home)
    def _():
        early_in[spot] = early_out[me]

    for k in range(side - 1):
        rows_forward(n, k, row_buf, gf, gl, gp)

    span_row = lax.broadcasted_iota(jnp.int32, (rows, span), 0)

    def read_state(g):
        maps = out_conv[:, g * states : (g + 1) * states].astype(BF16)

        def reduce_row(r, acc):
            block = held[r, g].astype(BF16)
            sums = lax.dot_general(
                maps, block, (((1,), (1,)), ((), ())), preferred_element_type=F32
            )
            return jnp.where(span_row == r, sums, acc)

        old_mix[:, g * span : (g + 1) * span] = lax.fori_loop(
            0, rows, reduce_row, jnp.zeros((rows, span), F32)
        )

    for read in reads:
        read.wait()
    for i in order[5:]:
        loads[i].start()
    for twin in twins[2:]:
        twin.start()
    for g in range(EARLY):
        read_state(g)
    rows_wait(n, row_buf, gs, gp)
    for i in (0, 1):
        loads[i].wait()
    for twin in twins[:2]:
        twin.wait_recv()
    arrived = [row_buf[f].reshape(hn * rows, half) for f in range(2)]
    for core in range(2):
        for k, w in enumerate((gw, vw)):
            made = sum(
                jnp.dot(
                    arrived[f], w[core, f * half : (f + 1) * half], preferred_element_type=F32
                )
                for f in range(2)
            )
            proj[core, :, k] = made.astype(BF16).reshape(hn, rows, piece)
    back_start(n, proj, back, rs, rr)

    @pl.when(at_home)
    def _():
        for k in reversed(range(side - 1)):
            for j in reversed(range(side)):
                p = plane_peer(j, side, line_peer(k, side))
                remote(early_out.at[p], early_in.at[spot], es, er, p, t).start()
        for j in reversed(range(1, side)):
            p = plane_peer(j, side)
            remote(early_out.at[p], early_in.at[spot], es, er, p, t).start()

    for g in range(EARLY, groups):
        read_state(g)

    back_wait(n, back, rs, rr)
    gate_rows = jnp.concatenate([back[j, 0] for j in range(n)], axis=1).astype(F32)
    value_rows = jnp.concatenate([back[j, 1] for j in range(n)], axis=1)
    value_conv = short_conv_in(v_past, value_rows, v_taps, v_next)
    scaled = step_wide * value_conv
    gate = jax.nn.silu(gate_rows)
    for g in range(groups):
        cut, maps = slice(g * span, (g + 1) * span), slice(g * states, (g + 1) * states)
        overlap = jnp.sum(in_conv[:, maps] * out_conv[:, maps], axis=-1, keepdims=True)
        mix = (
            decay_wide[:, cut] * old_mix[:, cut]
            + scaled[:, cut] * overlap
            + skip_wide[:, cut] * value_conv[:, cut]
        ) * gate[:, cut]
        mix = mix * lax.rsqrt(jnp.mean(mix * mix, axis=-1, keepdims=True) + EPSILON)
        mixed[:, cut] = (mix * group_gain[:, cut]).astype(BF16)

    rows_start(n, mixed, gath, as_, al, ap)
    hand = partner_copy(mixed, gath.at[t, spot], ns, nr)

    def keep():
        gath[t, spot] = mixed[...]

    by_home(n, keep, hand.start)

    top = scaled.astype(BF16).astype(F32)
    rest = scaled - top
    columns[...] = jnp.transpose(jnp.concatenate([top, rest, top], axis=0)).astype(BF16)
    map_row = lax.rem(lax.broadcasted_iota(jnp.int32, (3 * rows, states), 0), rows)

    def update_row(r, carry):
        decay_row = decays[pl.ds(r, 1), :]
        for g in range(groups):
            maps = in_conv[:, g * states : (g + 1) * states]
            high = maps.astype(BF16).astype(F32)
            triple = jnp.concatenate([high, high, maps - high], axis=0)
            picked = jnp.where(map_row == r, triple, 0.0).astype(BF16)
            grown = jnp.dot(
                columns[g * span : (g + 1) * span, :], picked, preferred_element_type=F32
            )
            for h in range(per_group):
                at = slice(h * head, (h + 1) * head)
                factor = decay_row[:, g * per_group + h : g * per_group + h + 1]
                held[r, g, at, :] = held[r, g, at, :] * factor + grown[at]
        return carry

    lax.fori_loop(0, BEFORE, update_row, 0)
    rows_forward(n, 0, gath, af, al, ap)
    rows_forward(n, 1, gath, af, al, ap)
    rows_forward(n, 2, gath, af, al, ap)
    lax.fori_loop(BEFORE, rows, update_row, 0)
    for i in range(5, 12):
        loads[i].wait()
    for twin in twins:
        twin.wait_send()
    for twin in twins[2:]:
        twin.wait_recv()
    rows_sent(n, row_buf, gs, gf)
    back_sent(n, back, rs, rr)
    by_home(
        n, lambda: bulk(early_in, hn - 1, es, er).wait_recv(),
        lambda: bulk(early_in, hn, es, er).wait_recv(),
    )

    @pl.when(at_home)
    def _():
        bulk(early_out, n - 1, es, er).wait_send()

    by_home(n, partner_copy(mixed, gath.at[1 - t, spot], ns, nr).wait_recv, hand.wait_send)
    rows_wait(n, gath, as_, ap)
    both = sum(
        jnp.dot(
            gath[f].reshape(hn * rows, inner), wm[f], preferred_element_type=F32
        ).astype(BF16).astype(F32)
        for f in range(2)
    ).astype(BF16).astype(F32)
    block = early_in[:, 0].reshape(hn * rows, piece).astype(F32)
    blocks[me] = (block + both).astype(BF16)

    def any_plane(block):
        return pp

    gather_start(n, blocks, ps, pr, any_plane)
    rows_sent(n, gath, as_, af)
    for k in range(side - 1):
        gather_forward(n, k, blocks, ps, pr, any_plane)
    bulk(blocks, n - side, ps, pp).wait_recv()
    stream = jnp.concatenate([blocks[j] for j in range(n)], axis=1)
    sx[...] = stream.reshape(hn, rows, width)
    give = partner_copy(sx.at[spot], own_rows, os_, or_)

    @pl.when(at_home)
    def _():
        own_rows[...] = sx[spot]
        give.start()

    ffn = rms_scale(stream, gain2[...]).astype(BF16)
    upper = lax.rem(lax.broadcasted_iota(jnp.int32, (hn * rows, 1), 0), rows) >= rows // 2
    pick = early_in[:, 1].reshape(hn * rows, piece)[:, : hn * rows]
    hidden = []
    for f in range(2):
        unit = (
            jax.nn.silu(jnp.dot(ffn, rg[f], preferred_element_type=F32))
            * jnp.dot(ffn, ru[f], preferred_element_type=F32)
        ).astype(BF16)
        hidden.append(jnp.dot(pick, unit, preferred_element_type=F32).astype(BF16))
    for core in range(2):
        outs = [
            sum(
                jnp.dot(
                    hidden[f], rd[f, :, q * quarter : (q + 1) * quarter],
                    preferred_element_type=F32,
                )
                for f in range(2)
            )
            for q in (2 * core, 2 * core + 1)
        ]
        ret[core] = jnp.where(upper, outs[1], outs[0]).astype(BF16).reshape(hn, rows, quarter)
    back_start(n, ret, home, fs, fr)
    by_home(n, give.wait_send, give.wait_recv)
    mine = own_rows[...]
    mine_ffn = rms_scale(mine, gain2[...]).astype(BF16)
    shared_hidden = (
        jax.nn.silu(jnp.dot(mine_ffn, cg[...], preferred_element_type=F32))
        * jnp.dot(mine_ffn, cu[...], preferred_element_type=F32)
    ).astype(BF16)
    shared = jnp.dot(shared_hidden, cd[...], preferred_element_type=F32)
    share[...] = far_half(shared)
    swap = partner_copy(share, theirs, hs, hr)
    swap.start()
    bulk(blocks, n - 1, ps, pp).wait_send()
    swap.wait_recv()
    base = own_half(mine.astype(F32)) + (own_half(shared) + theirs[...])
    swap.wait_send()
    back_wait(n, home, fs, fr)
    routed = jnp.dot(
        combine, home[...].reshape(n * rows, quarter).astype(F32),
        precision=lax.Precision.HIGHEST, preferred_element_type=F32,
    )
    routed = jnp.concatenate([routed[:rows], routed[rows:]], axis=1)
    half_out[...] = (base + routed).astype(BF16)
    last = partner_copy(half_out, half_in, ls, lr)
    last.start()
    back_sent(n, home, fs, fr)
    last.wait_recv()
    near, far = half_out[...], half_in[...]
    result[:, :half] = jnp.where(t == 0, near, far)
    result[:, half:] = jnp.where(t == 0, far, near)
    last.wait_send()


def mixer_step(n, capacity, small, state, weights):
    rows, width = small[0].shape
    half = width // 2
    piece = weights[0].shape[1]
    inner = n * piece
    groups, span, _ = state.shape[1:]
    vmem, hbm = pl.BlockSpec(memory_space=pltpu.VMEM), pl.BlockSpec(memory_space=pl.ANY)
    dma = pltpu.SemaphoreType.DMA
    many, twice = dma((level(n),)), dma((2 * level(n),))
    hn = n // 2
    heads = small[2].shape[1]
    return pl.pallas_call(
        functools.partial(step_kernel, n, capacity),
        out_shape=(
            pltpu.VMEM((rows, width), BF16),
            pltpu.VMEM(state.shape, F32),
            pltpu.VMEM(small[8].shape, BF16),
            pltpu.VMEM(small[9].shape, BF16),
            pltpu.VMEM(small[10].shape, BF16),
        ),
        in_specs=[hbm] * (len(small) + 1 + len(weights)),
        out_specs=(vmem,) * 5,
        scratch_shapes=[pltpu.VMEM(a.shape, a.dtype) for a in small]
        + [
            pltpu.VMEM((rows, half), BF16),
            pltpu.VMEM((2, hn, rows, half), BF16),
            pltpu.VMEM((2, hn, 2, rows, piece), BF16),
            pltpu.VMEM((n, 2, rows, piece), BF16),
            pltpu.VMEM((rows, inner), F32),
            pltpu.VMEM((rows, heads), F32),
            pltpu.VMEM((inner, 3 * rows), BF16),
            pltpu.VMEM((rows, inner), BF16),
            pltpu.VMEM((2, hn, rows, inner), BF16),
            pltpu.VMEM((n, 2, rows, piece), BF16),
            pltpu.VMEM((hn, 2, rows, piece), BF16),
            pltpu.VMEM((n, hn * rows, piece), BF16),
            pltpu.VMEM((hn, rows, width), BF16),
            pltpu.VMEM((rows, width), BF16),
            pltpu.VMEM((2, hn, rows, half // 2), BF16),
            pltpu.VMEM((n, rows, half // 2), BF16),
            pltpu.VMEM((rows, half), F32),
            pltpu.VMEM((rows, half), F32),
            pltpu.VMEM((rows, half), BF16),
            pltpu.VMEM((rows, half), BF16),
        ]
        + [
            pltpu.VMEM((2, *w.shape) if i in TWIN else w.shape, BF16)
            for i, w in enumerate(weights)
        ]
        + [dma((len(weights),)), dma((len(small),)), dma, dma((len(TWIN),)), dma((len(TWIN),))]
        + [dma, many, twice, dma] + [dma] * 4 + [dma, many, twice, dma] + [dma] * 2
        + [dma, many, dma] + [dma] * 8,
        compiler_params=pltpu.CompilerParams(
            collective_id=0, has_side_effects=True, vmem_limit_bytes=54 << 20
        ),
    )(*[pltpu.with_memory_space_constraint(a, pltpu.HBM) for a in (*small, state, *weights)])


def store_kernel(count, *refs):
    inputs, outputs, sems = refs[:count], refs[count : 2 * count], refs[2 * count]
    rows = inputs[0].shape[0]
    copies = [
        pltpu.make_async_copy(inputs[0].at[r], outputs[0].at[r], sems.at[r]) for r in range(rows)
    ]
    for k in range(1, count):
        copies.append(pltpu.make_async_copy(inputs[k], outputs[k], sems.at[rows + k - 1]))
    for copy in copies:
        copy.start()
    for copy in copies:
        copy.wait()


def store(*arrays):
    count = len(arrays)
    return pl.pallas_call(
        functools.partial(store_kernel, count),
        out_shape=tuple(jax.ShapeDtypeStruct(a.shape, a.dtype) for a in arrays),
        in_specs=[pl.BlockSpec(memory_space=pltpu.VMEM)] * count,
        out_specs=(pl.BlockSpec(memory_space=pl.ANY),) * count,
        scratch_shapes=[pltpu.SemaphoreType.DMA((arrays[0].shape[0] + count - 1,))],
        compiler_params=pltpu.CompilerParams(vmem_limit_bytes=1 << 20),
    )(*[pltpu.with_memory_space_constraint(a, pltpu.VMEM) for a in arrays])


def fast_shards(
    tokens,
    mixer_norm_gain,
    gate_projection_weight,
    value_projection_weight,
    input_projection_weight,
    output_projection_weight,
    step_projection_weight,
    head_step_bias,
    head_decay_rate,
    extra_log_decay,
    value_taps,
    input_taps,
    output_taps,
    prior_values,
    prior_input_maps,
    prior_output_maps,
    head_skip_gain,
    group_norm_gain,
    mixer_output_weight,
    recurrent_state,
    expert_norm_gain,
    routes,
    chosen_expert_weight,
    routed_gate_weight,
    routed_up_weight,
    routed_down_weight,
    common_gate_weight,
    common_up_weight,
    common_down_weight,
):
    seq_rows, model_width = tokens.shape
    ep_count = lax.axis_size("ep")
    capacity = (seq_rows * routes.shape[1] + ep_count - 1) // ep_count + 1

    def one_row(vector):
        return vector.reshape(1, -1)

    def flat(weight):
        return weight.reshape(model_width, -1)

    states = recurrent_state.shape[3]
    group_count = input_projection_weight.shape[1] // states
    small = (
        tokens, one_row(mixer_norm_gain), one_row(head_step_bias), one_row(head_decay_rate),
        extra_log_decay, value_taps, input_taps, output_taps,
        prior_values.transpose(1, 0, 2), prior_input_maps.transpose(1, 0, 2),
        prior_output_maps.transpose(1, 0, 2), one_row(head_skip_gain), one_row(group_norm_gain),
        one_row(expert_norm_gain), routes, chosen_expert_weight,
    )
    weights = (
        flat(gate_projection_weight), flat(value_projection_weight), input_projection_weight,
        output_projection_weight, step_projection_weight.T, mixer_output_weight,
        common_gate_weight, common_up_weight, common_down_weight,
        routed_gate_weight.reshape(routed_gate_weight.shape[1:]),
        routed_up_weight.reshape(routed_up_weight.shape[1:]),
        routed_down_weight.reshape(routed_down_weight.shape[1:]),
    )
    result, state_next, next_value, next_input, next_output = mixer_step(
        ep_count, capacity, small,
        recurrent_state.reshape(seq_rows, group_count, -1, states), weights,
    )
    state_next, result, next_value, next_input, next_output = store(
        state_next, result, next_value, next_input, next_output
    )
    return (
        result,
        state_next.reshape(recurrent_state.shape),
        next_value.transpose(1, 0, 2),
        next_input.transpose(1, 0, 2),
        next_output.transpose(1, 0, 2),
    )


def fits_kernels(rows, n, tp, gate_w, mix_w, routes, routed_w):
    if tp != 2 or routed_w.shape[0] != 1 or rows != 8:
        return False
    capacity = (rows * routes.shape[1] + n - 1) // n + 1
    return level(n) ** 2 == n and n // 2 * rows <= mix_w.shape[1] == gate_w.shape[2] and gate_w.shape[2] % 128 == 0 and mix_w.shape[1] % 128 == 0 and 2 * capacity == rows


def shards(
    tokens,
    mixer_norm_gain,
    gate_projection_weight,
    value_projection_weight,
    input_projection_weight,
    output_projection_weight,
    step_projection_weight,
    head_step_bias,
    head_decay_rate,
    extra_log_decay,
    value_taps,
    input_taps,
    output_taps,
    prior_values,
    prior_input_maps,
    prior_output_maps,
    head_skip_gain,
    group_norm_gain,
    mixer_output_weight,
    recurrent_state,
    expert_norm_gain,
    routes,
    chosen_expert_weight,
    routed_gate_weight,
    routed_up_weight,
    routed_down_weight,
    common_gate_weight,
    common_up_weight,
    common_down_weight,
):
    seq_rows, model_width = tokens.shape
    ep_count = lax.axis_size("ep")
    tp_count = lax.axis_size("tp")
    if fits_kernels(seq_rows, ep_count, tp_count, gate_projection_weight, mixer_output_weight, routes, routed_gate_weight):
        return fast_shards(
            tokens, mixer_norm_gain, gate_projection_weight, value_projection_weight,
            input_projection_weight, output_projection_weight, step_projection_weight,
            head_step_bias, head_decay_rate, extra_log_decay, value_taps, input_taps,
            output_taps, prior_values, prior_input_maps, prior_output_maps, head_skip_gain,
            group_norm_gain, mixer_output_weight, recurrent_state, expert_norm_gain, routes,
            chosen_expert_weight, routed_gate_weight, routed_up_weight, routed_down_weight,
            common_gate_weight, common_up_weight, common_down_weight,
        )
    tp_place = lax.axis_index("tp")
    normed = rms_scale(tokens, mixer_norm_gain).astype(jnp.bfloat16)
    both_pieces = jnp.concatenate(
        [
            gate_projection_weight.reshape(model_width, -1),
            value_projection_weight.reshape(model_width, -1),
        ],
        axis=1,
    )
    piece_width = both_pieces.shape[1] // 2
    projected = jnp.dot(
        lax.all_gather(normed, "ep", axis=0, tiled=True),
        both_pieces,
        preferred_element_type=jnp.float32,
    ).astype(jnp.bfloat16)
    returned = lax.all_to_all(projected, "ep", split_axis=0, concat_axis=1, tiled=True).reshape(
        seq_rows, ep_count, 2, piece_width
    )
    gate_rows = returned[:, :, 0].reshape(seq_rows, -1)
    value_rows = returned[:, :, 1].reshape(seq_rows, -1)
    input_rows = jnp.dot(
        normed, input_projection_weight, preferred_element_type=jnp.float32
    ).astype(jnp.bfloat16)
    output_rows = jnp.dot(
        normed, output_projection_weight, preferred_element_type=jnp.float32
    ).astype(jnp.bfloat16)
    step_raw = jnp.dot(normed, step_projection_weight, preferred_element_type=jnp.float32)
    value_conv, next_value = short_conv(prior_values, value_rows, value_taps)
    input_conv, next_input = short_conv(prior_input_maps, input_rows, input_taps)
    output_conv, next_output = short_conv(prior_output_maps, output_rows, output_taps)
    timestep_size = jax.nn.softplus(step_raw + head_step_bias)
    step_decay = jnp.exp(-timestep_size * head_decay_rate + extra_log_decay)
    state_next, mixed_flat = state_step(
        recurrent_state,
        value_conv,
        input_conv,
        output_conv,
        timestep_size,
        step_decay,
        head_skip_gain,
    )
    mixer_rows = gated_norm(mixed_flat, gate_rows, group_norm_gain, D_INNER // GROUPS)
    partial_mix = jnp.dot(
        lax.all_gather(mixer_rows, "ep", axis=0, tiled=True),
        mixer_output_weight,
        preferred_element_type=jnp.float32,
    )
    mix_share = lax.psum_scatter(
        partial_mix.reshape(ep_count, seq_rows, -1).astype(jnp.bfloat16),
        "tp",
        scatter_dimension=1,
        tiled=True,
    )
    moved_mix = lax.all_to_all(mix_share, "ep", split_axis=0, concat_axis=2, tiled=True)
    mixed_out = lax.all_gather(moved_mix, "tp", axis=1, tiled=True).reshape(seq_rows, model_width)
    stream = (tokens.astype(jnp.float32) + mixed_out.astype(jnp.float32)).astype(jnp.bfloat16)
    ffn_rows = rms_scale(stream, expert_norm_gain).astype(jnp.bfloat16)
    shared_hidden = (
        jax.nn.silu(jnp.dot(ffn_rows, common_gate_weight, preferred_element_type=jnp.float32))
        * jnp.dot(ffn_rows, common_up_weight, preferred_element_type=jnp.float32)
    ).astype(jnp.bfloat16)
    shared_out = lax.psum(
        jnp.dot(shared_hidden, common_down_weight, preferred_element_type=jnp.float32).astype(
            jnp.bfloat16
        ),
        "tp",
    ).astype(jnp.float32)
    exp_local = routed_gate_weight.shape[0]
    expert_total = exp_local * ep_count
    topk_count = routes.shape[1]
    capacity = (seq_rows * topk_count + expert_total - 1) // expert_total + 1
    slot_count = expert_total * capacity
    expert_ids = jnp.arange(expert_total, dtype=jnp.int32)
    flat_routes = routes.reshape(-1)
    onehot = (flat_routes[:, None] == expert_ids[None, :]).astype(jnp.int32)
    slot_ids = jnp.sum((jnp.cumsum(onehot, axis=0) - onehot) * onehot, axis=1)
    positions = flat_routes * capacity + slot_ids
    matches = (jnp.arange(slot_count, dtype=jnp.int32)[:, None] == positions[None, :]).reshape(
        slot_count, seq_rows, topk_count
    )
    dispatch_mat = jnp.sum(matches.astype(jnp.float32), axis=2).astype(jnp.bfloat16)
    combine_mat = jnp.sum(jnp.where(matches, chosen_expert_weight[None], 0.0), axis=2)
    outgoing = jnp.dot(dispatch_mat, ffn_rows, preferred_element_type=jnp.float32).astype(
        jnp.bfloat16
    )
    outgoing = outgoing.reshape(ep_count, exp_local, capacity, model_width)
    half_width = model_width // tp_count
    own_cols = lax.dynamic_slice_in_dim(outgoing, tp_place * half_width, half_width, 3)
    full_rows = lax.all_gather(
        lax.all_to_all(own_cols, "ep", split_axis=0, concat_axis=0, tiled=True),
        "tp",
        axis=3,
        tiled=True,
    )
    partial_out = expert_partial(
        full_rows, routed_gate_weight, routed_up_weight, routed_down_weight
    )
    share_out = lax.psum_scatter(
        partial_out.astype(jnp.bfloat16), "tp", scatter_dimension=3, tiled=True
    )
    back_half = lax.all_to_all(share_out, "ep", split_axis=0, concat_axis=0, tiled=True)
    routed_half = lax.dot_general(
        combine_mat,
        back_half.reshape(slot_count, half_width).astype(jnp.float32),
        (((0,), (0,)), ((), ())),
        precision=lax.Precision.HIGHEST,
    )
    routed = lax.all_gather(routed_half.astype(jnp.bfloat16), "tp", axis=1, tiled=True).astype(
        routed_half.dtype
    )
    result = (stream.astype(jnp.float32) + shared_out + routed).astype(jnp.bfloat16)
    return (result, state_next, next_value, next_input, next_output)


def solution(mesh):
    return jax.shard_map(
        shards,
        mesh=mesh,
        in_specs=(
            P("ep", None),
            P(),
            P(None, "tp", "ep"),
            P(None, "tp", "ep"),
            P(None, "tp"),
            P(None, "tp"),
            P(None, "tp"),
            P("tp"),
            P("tp"),
            P("ep", "tp"),
            P(None, "tp"),
            P(None, "tp"),
            P(None, "tp"),
            P("ep", None, "tp"),
            P("ep", None, "tp"),
            P("ep", None, "tp"),
            P("tp"),
            P("tp"),
            P("tp", "ep"),
            P("ep", "tp", None, None),
            P(),
            P("ep", None),
            P("ep", None),
            P("ep", None, "tp"),
            P("ep", None, "tp"),
            P("ep", "tp", None),
            P(None, "tp"),
            P(None, "tp"),
            P("tp", None),
        ),
        out_specs=(
            P("ep", None),
            P("ep", "tp", None, None),
            P("ep", None, "tp"),
            P("ep", None, "tp"),
            P("ep", None, "tp"),
        ),
        check_vma=False,
    )
```
